1024 devices in a mesh: kv: 128 (over z, y), tp: 8 (over x, core).
Axes of the slice: x: 4, y: 8, z: 16, core: 2. Of those that a mesh axis runs over, the one named last changes fastest.
Arguments:
- queries: bfloat16 [16384, 1024], P('kv', 'tp'), may hold values from -6 to 6
- keys: bfloat16 [16384, 512], P('kv', 'tp'), may hold values from -6 to 6
- values: bfloat16 [16384, 512], P('kv', 'tp'), may hold values from -6 to 6
- hidden: bfloat16 [16384, 2048], P('kv'), may hold values from -6 to 6
- log_sums: float32 [2, 16384, 16], P(None, 'kv', 'tp'), may hold values from -1 to 12
- gates: float32 [2, 16384, 16], P(None, 'kv', 'tp'), may hold values from 0.1 to 0.9
- branch_out: bfloat16 [2, 16384, 1024], P(None, 'kv', 'tp'), may hold values from -6 to 6
- cotangent: bfloat16 [16384, 1024], P('kv', 'tp'), may hold values from -6 to 6
- chosen: int32 [128, 8, 48], P(None, 'tp'), may hold values from -1 to 511, as said below
Outputs:
- grad_queries: float32 [16384, 1024], P('kv', 'tp')
- grad_keys: float32 [16384, 512], P('kv', 'tp')
- grad_values: float32 [16384, 512], P('kv', 'tp')
- grad_weight: float32 [2048, 1024], P('kv', 'tp')
The draws below stay inside these ranges and needn't reach their ends.
Inputs may be any that keep to these rules, and one draw needn't show every extreme that they name: `chosen`: each list holds global block numbers or -1. All live entries of one list name blocks of distinct owners, owner = entry // 4, none later than the list's range; list d holds min(48, d + 1) live entries, and they come first.
All inputs are finite; a program needn't handle non-finite values.
Results may differ from the reference program's by a relative error of at most 0.0055.
Values may be sent and summed in bfloat16 or wider, within the bound.
No kernel may reach another device: no remote copies, remote signals or barrier semaphores. Data moves between devices by JAX's collectives and lax.ppermute only.
A program may use at most 32 MiB of HBM per device.

```python
import jax
import jax.numpy as jnp
from jax import lax

D = 2048
HQ = 16
KVG = 8
DH = 64
BLK = 32
TOPN = 12
SUB = 4
CMP = 32
TOK_DEV = 128
TOKENS = 16384


def draw_log_sums(key, part):
    position = jnp.arange(TOKENS, dtype=jnp.int32)
    device = position // TOK_DEV
    sub_index = position % TOK_DEV // (TOK_DEV // SUB)
    summary_seen = jnp.maximum((position + 1) // CMP, 1).astype(jnp.float32)
    live_here = jnp.clip(jnp.minimum(SUB * TOPN, device + 1) - sub_index * TOPN, 1, TOPN)
    block_seen = (live_here * BLK).astype(jnp.float32)
    base = jnp.stack([jnp.log(summary_seen), jnp.log(block_seen) + 0.5])[:, :, None]
    noise = jnp.clip(jax.random.normal(key, (2, TOKENS, HQ), jnp.float32) * 0.3, -0.9, 0.9)
    return base + noise


def draw_chosen(key, part):
    blocks_all = TOKENS // TOK_DEV
    per_block = TOK_DEV // BLK
    nsel = SUB * TOPN
    taken_count = min(nsel, blocks_all)
    first_key = jax.random.fold_in(key, 11)
    second_key = jax.random.fold_in(key, 23)
    device = jnp.arange(blocks_all, dtype=jnp.int32)[:, None, None]
    owner = jnp.arange(blocks_all, dtype=jnp.int32)[None, None, :]
    random_part = jax.random.randint(first_key, (blocks_all, KVG, blocks_all), 0, 1000) * blocks_all + owner
    forced = (owner == device) | (owner == device - 1) | (owner == device - blocks_all // 2) | (owner == 0)
    score = jnp.where(owner <= device, random_part + forced.astype(jnp.int32) * (2000 * blocks_all), -1)
    top_score, picks = lax.top_k(score, taken_count)
    inner = jax.random.randint(second_key, (blocks_all, KVG, taken_count), 0, per_block - 1)
    far_pick = (picks == device - blocks_all // 2) & (device >= blocks_all // 2)
    inner = jnp.where(far_pick, per_block - 1, inner)
    listing = jnp.where(top_score >= 0, picks * per_block + inner, -1).astype(jnp.int32)
    if nsel > taken_count:
        filler = jnp.full((blocks_all, KVG, nsel - taken_count), -1, jnp.int32)
        listing = jnp.concatenate([listing, filler], -1)
    return listing


def block_levels(own_key, dims, pieces, low, high):
    def one(dim, shards_of):
        steps = jax.random.uniform(jax.random.fold_in(jax.random.fold_in(own_key, 6), dim), (shards_of,), jnp.float32, low / len(pieces), high / len(pieces))
        return jnp.repeat(jnp.exp(steps), dims[dim] // shards_of).reshape((-1,) + (1,) * (len(dims) - dim - 1))

    factor_of = one(*pieces[0])
    for cut in pieces[1:]:
        factor_of = factor_of * one(*cut)
    return factor_of


def gaussian(key, dims, width, bound, pieces=(), kind=jnp.bfloat16):
    drawn = jax.random.normal(key, dims, jnp.float32) * width
    if len(pieces) > 0:
        drawn = block_levels(key, dims, pieces, -0.22, 0.18) * drawn
    return jnp.clip(drawn, min=-bound, max=bound).astype(kind)


def setup_inputs(seed: int = 0) -> dict:
    streams_of = jax.random.split(jax.random.key(seed), 10)
    queries = gaussian(streams_of[0], (TOKENS, HQ * DH), 1.0, 6.0, ((0, 128), (1, 8)))
    keys = gaussian(streams_of[1], (TOKENS, KVG * DH), 1.0, 6.0, ((0, 128), (1, 8)))
    values = gaussian(streams_of[2], (TOKENS, KVG * DH), 1.0, 6.0, ((0, 128), (1, 8)))
    hidden = gaussian(streams_of[3], (TOKENS, D), 1.0, 6.0, ((0, 128),))
    log_sums = draw_log_sums(jax.random.fold_in(streams_of[9], 71), 0)
    gates = jnp.clip(0.1 + 0.79999997 * jax.random.uniform(streams_of[5], (2, TOKENS, HQ), jnp.float32) ** block_levels(streams_of[5], (2, TOKENS, HQ), ((1, 128), (2, 8)), -0.2, 0.2), 0.1, 0.9)
    branch_out = gaussian(streams_of[6], (2, TOKENS, HQ * DH), 1.0, 6.0, ((1, 128), (2, 8)))
    cotangent = gaussian(streams_of[7], (TOKENS, HQ * DH), 1.0, 6.0, ((0, 128), (1, 8)))
    chosen = draw_chosen(jax.random.fold_in(streams_of[9], 71), 0)
    return {"queries": queries, "keys": keys, "values": values, "hidden": hidden, "log_sums": log_sums, "gates": gates, "branch_out": branch_out, "cotangent": cotangent, "chosen": chosen}


def branch_grads(query_rows, key_rows, value_rows, seen, log_rows, delta_rows, cot_rows, scale):
    wide = jnp.float32
    scores = jnp.einsum('tgre,gme->grtm', query_rows.astype(wide), key_rows.astype(wide)) * scale
    log_here = jnp.transpose(log_rows, (1, 2, 0))[..., None]
    delta_here = jnp.transpose(delta_rows, (1, 2, 0))[..., None]
    probs = jnp.where(seen[:, None], jnp.exp(scores - log_here), 0.0)
    probs_low = lax.optimization_barrier(probs.astype(jnp.bfloat16)).astype(wide)
    value_grad = jnp.einsum('grtm,tgre->gme', probs_low, cot_rows.astype(wide))
    prob_grad = jnp.einsum('tgre,gme->grtm', cot_rows.astype(wide), value_rows.astype(wide))
    score_grad = probs * (prob_grad - delta_here)
    score_low = lax.optimization_barrier(score_grad.astype(jnp.bfloat16)).astype(wide)
    query_grad = jnp.einsum('grtm,gme->tgre', score_low, key_rows.astype(wide)) * scale
    key_grad = jnp.einsum('grtm,tgre->gme', score_low, query_rows.astype(wide)) * scale
    return query_grad, key_grad, value_grad


def reference(queries, keys, values, hidden, log_sums, gates, branch_out, cotangent, chosen):
    wide = jnp.float32
    group_heads = HQ // KVG
    nsel = SUB * TOPN
    qrows = TOK_DEV // SUB
    scale = DH ** -0.5
    summary_count = TOKENS // CMP
    grads_each = jax.vmap(branch_grads, in_axes=(0, 0, 0, 0, 0, 0, 0, None))
    query_all = queries.reshape(TOKENS, KVG, group_heads, DH)
    gated = gates[..., None] * cotangent.reshape(TOKENS, HQ, DH).astype(wide)[None]
    delta_all = jnp.sum(gated * branch_out.reshape(2, TOKENS, HQ, DH).astype(wide), -1)
    delta_all = delta_all.reshape(2, TOKENS, KVG, group_heads)
    gated_low = gated.astype(jnp.bfloat16).reshape(2, TOKENS, KVG, group_heads, DH)
    log_all = log_sums.reshape(2, TOKENS, KVG, group_heads)
    sum_keys = jnp.mean(keys.reshape(summary_count, CMP, KVG, DH).astype(wide), 1).astype(jnp.bfloat16)
    sum_values = jnp.mean(values.reshape(summary_count, CMP, KVG, DH).astype(wide), 1).astype(jnp.bfloat16)
    sum_keys = jnp.transpose(sum_keys, (1, 0, 2))
    sum_values = jnp.transpose(sum_values, (1, 0, 2))
    key_blocks = keys.reshape(TOKENS // BLK, BLK, KVG, DH)
    value_blocks = values.reshape(TOKENS // BLK, BLK, KVG, DH)
    group_index = jnp.arange(KVG, dtype=jnp.int32)[:, None]
    summary_end = jnp.arange(summary_count, dtype=jnp.int32) * CMP + CMP - 1

    def by_sub(array):
        rest = array.shape[3:]
        moved = array.reshape((KVG, SUB, TOPN * BLK) + rest)
        return jnp.swapaxes(moved, 0, 1)

    def step(carry, index):
        sel_keys, sel_values, summ_keys, summ_values = carry
        start = index * TOK_DEV
        query_here = lax.dynamic_slice_in_dim(query_all, start, TOK_DEV, 0)
        cot_here = lax.dynamic_slice_in_dim(gated_low, start, TOK_DEV, 1)
        log_here = lax.dynamic_slice_in_dim(log_all, start, TOK_DEV, 1)
        delta_here = lax.dynamic_slice_in_dim(delta_all, start, TOK_DEV, 1)
        position = start + jnp.arange(TOK_DEV, dtype=jnp.int32)
        summary_seen = (summary_end[None, :] <= position[:, None])[None]
        query_sum, key_sum, value_sum = branch_grads(query_here, sum_keys, sum_values, summary_seen,
                                                     log_here[0], delta_here[0], cot_here[0], scale)
        listing = lax.dynamic_index_in_dim(chosen, index, 0, keepdims=False)
        live = listing >= 0
        safe = jnp.maximum(listing, 0)
        picked_keys = by_sub(key_blocks[safe, :, group_index, :])
        picked_values = by_sub(value_blocks[safe, :, group_index, :])
        key_position = by_sub(safe[..., None] * BLK + jnp.arange(BLK, dtype=jnp.int32))
        live_rows = by_sub(jnp.broadcast_to(live[..., None], (KVG, nsel, BLK)))
        sub_position = position.reshape(SUB, qrows)
        block_seen = live_rows[:, :, None, :] & (key_position[:, :, None, :] <= sub_position[:, None, :, None])
        query_sel, key_sel, value_sel = grads_each(
            query_here.reshape(SUB, qrows, KVG, group_heads, DH), picked_keys, picked_values, block_seen,
            log_here[1].reshape(SUB, qrows, KVG, group_heads), delta_here[1].reshape(SUB, qrows, KVG, group_heads),
            cot_here[1].reshape(SUB, qrows, KVG, group_heads, DH), scale)
        query_sel = query_sel.reshape(TOK_DEV, KVG, group_heads, DH)
        key_sel = jnp.swapaxes(key_sel, 0, 1).reshape(KVG, nsel, BLK, DH)
        value_sel = jnp.swapaxes(value_sel, 0, 1).reshape(KVG, nsel, BLK, DH)
        weight_live = live[..., None, None].astype(wide)
        sel_keys = sel_keys.at[safe, :, group_index, :].add(key_sel * weight_live)
        sel_values = sel_values.at[safe, :, group_index, :].add(value_sel * weight_live)
        return (sel_keys, sel_values, summ_keys + key_sum, summ_values + value_sum), query_sum + query_sel

    start_state = (jnp.zeros((TOKENS // BLK, BLK, KVG, DH), wide), jnp.zeros((TOKENS // BLK, BLK, KVG, DH), wide),
                   jnp.zeros((KVG, summary_count, DH), wide), jnp.zeros((KVG, summary_count, DH), wide))
    final_state, query_blocks = lax.scan(step, start_state, jnp.arange(TOKENS // TOK_DEV, dtype=jnp.int32))
    sel_keys, sel_values, summ_keys, summ_values = final_state
    grad_queries = query_blocks.reshape(TOKENS, HQ * DH)
    grad_keys = sel_keys.reshape(TOKENS, KVG, DH) + jnp.repeat(jnp.transpose(summ_keys, (1, 0, 2)), CMP, axis=0) / CMP
    grad_values = sel_values.reshape(TOKENS, KVG, DH) + jnp.repeat(jnp.transpose(summ_values, (1, 0, 2)), CMP, axis=0) / CMP
    grad_weight = jnp.dot(hidden.T, grad_queries.astype(jnp.bfloat16), preferred_element_type=jnp.float32)
    return (grad_queries, grad_keys.reshape(TOKENS, KVG * DH), grad_values.reshape(TOKENS, KVG * DH), grad_weight)
```

```python
import jax
import jax.numpy as jnp
from jax import lax
from jax.experimental import pallas as pl
from jax.experimental.pallas import tpu as pltpu
from jax.sharding import Mesh
from jax.sharding import PartitionSpec as P

DH = 64
BLK = 32
TOPN = 12
SUB = 4
CMP = 32
KV = ("kv_0", "kv_1")
FAR = 1 << 30
WIDE = jnp.float32
LOW = jnp.bfloat16
ROWS = 40


def dot(a, b, ca, cb):
    return lax.dot_general(a, b, (((ca,), (cb,)), ((), ())), preferred_element_type=WIDE)


def outbound_kernel(wanted_ref, keys_ref, values_ref, out_ref, pairs_ref):
    pairs = jnp.concatenate([keys_ref[...], values_ref[...]], -1).astype(WIDE)
    pairs_ref[...] = pairs.astype(LOW).reshape(pairs_ref.shape)
    blocks = pairs_ref.shape[0]
    means = jnp.mean(pairs.reshape(blocks, CMP, 2 * DH), 1)
    tail = jnp.concatenate([means, jnp.zeros((ROWS - BLK - blocks, 2 * DH), WIDE)], 0).astype(LOW)

    def one(d, carry):
        out_ref[d, :BLK, :] = pairs_ref[wanted_ref[d]]
        out_ref[d, BLK:, :] = tail
        return carry

    lax.fori_loop(0, out_ref.shape[0], one, 0, unroll=8)


def main_kernel(own_ref, msum_ref, msel_ref, ldsum_ref, ldsel_ref, relsum_ref, relsel_ref, arr_ref,
                dq_ref, ret_ref, kv_ref):
    rows = dq_ref.shape[0]
    owners = arr_ref.shape[0]
    wide = ROWS - BLK
    scale = DH ** (-0.5)
    both = 2 * rows

    def grads(m, kv, seen, ld):
        half = m.shape[0] // 2
        sd = dot(m, kv, 1, 1)
        probs = jnp.where(seen, jnp.exp(sd[:half] - ld[:, :1]), 0.0)
        ds = (probs * (sd[half:] - ld[:, 1:2])).astype(LOW)
        weights = jnp.concatenate([ds, probs.astype(LOW)], 0)
        return dot(ds, kv, 1, 0), dot(weights, m, 0, 0)

    m = msum_ref[...]
    ld = ldsum_ref[...]
    row_at = lax.broadcasted_iota(jnp.int32, (both, 1), 0) & (rows - 1)
    step = 32
    dq_sum = jnp.zeros((both, 2 * DH), WIDE)
    for first in range(0, owners, step):
        kv = arr_ref[first:first + step, BLK:, :].astype(WIDE).reshape(step * wide, 2 * DH).astype(LOW)
        seen = relsum_ref[:, first * wide:(first + step) * wide] <= row_at
        dq_part, kv_grad = grads(m, kv, seen, ld)
        dq_sum += dq_part
        ret_ref[first:first + step, BLK:, :] = kv_grad.reshape(step, wide, 2 * DH).astype(LOW)
    sub_rows = rows // SUB
    sub_at = lax.broadcasted_iota(jnp.int32, (2 * sub_rows, 1), 0) & (sub_rows - 1)
    for s in range(SUB):
        for i in range(TOPN):
            owner = jnp.maximum(own_ref[s * TOPN + i], 0)
            kv_ref[i * BLK:(i + 1) * BLK, :] = arr_ref[owner, :BLK, :]
        kv = kv_ref[...]
        seen = relsel_ref[s:s + 1, :] <= sub_at + s * sub_rows
        dq_part, kv_grad = grads(msel_ref[s], kv, seen, ldsel_ref[s])
        low = kv_grad.astype(LOW)
        for i in range(TOPN):
            owner = own_ref[s * TOPN + i]

            @pl.when(owner >= 0)
            def _(owner=owner, i=i):
                ret_ref[owner, :BLK, :] = low[i * BLK:(i + 1) * BLK]

        at = s * sub_rows
        for h in range(2):
            total = dq_sum[h * rows + at:h * rows + at + sub_rows, :DH]
            total = total + dq_part[h * sub_rows:(h + 1) * sub_rows, :DH]
            dq_ref[at:at + sub_rows, h * DH:(h + 1) * DH] = total * scale


def weight_kernel(hidden_ref, dq_ref, out_ref):
    low = dq_ref[...].astype(LOW)
    fast, per_slow, cols = out_ref.shape
    slow = hidden_ref.shape[1] // (fast * 16)
    span = fast * 16
    for z in range(slow):
        part = dot(hidden_ref[:, z * span:(z + 1) * span], low, 0, 0).astype(LOW)
        for y in range(fast):
            out_ref[y, z * 16:(z + 1) * 16, :] = part[y * 16:(y + 1) * 16]


def inbound_kernel(chosen_ref, in_ref, gk_ref, gv_ref):
    per_block = gk_ref.shape[0] // BLK

    def one(d, carry):
        sums, tail = carry
        here = in_ref[d, :BLK, :].astype(WIDE)
        pick = chosen_ref[d]
        sums = tuple(sums[b] + jnp.where(pick == b, here, 0.0) for b in range(per_block))
        return sums, tail + in_ref[d, BLK:, :].astype(WIDE)

    zero = jnp.zeros((BLK, 2 * DH), WIDE)
    start = ((zero,) * per_block, jnp.zeros((ROWS - BLK, 2 * DH), WIDE))
    sums, tail = lax.fori_loop(0, in_ref.shape[0], one, start, unroll=4)
    for b in range(per_block):
        total = sums[b] + tail[b:b + 1] * (1.0 / CMP)
        gk_ref[b * BLK:(b + 1) * BLK, :] = total[:, :DH]
        gv_ref[b * BLK:(b + 1) * BLK, :] = total[:, DH:]


def vmem():
    return pl.BlockSpec(memory_space=pltpu.VMEM)


def smem():
    return pl.BlockSpec(memory_space=pltpu.SMEM)


def shards(queries, keys, values, hidden, log_sums, gates, branch_out, cotangent, chosen):
    rows = queries.shape[0]
    heads = queries.shape[1] // DH
    per_block = rows // BLK
    owners = chosen.shape[0]
    nsel = chosen.shape[2]
    sub_rows = rows // SUB
    slow = lax.axis_size(KV[0])
    fast = lax.axis_size(KV[1])
    place = lax.axis_index(KV)
    lists = chosen[:, 0]
    hits = (lists >= 0) & (lists // per_block == place)
    wanted = jnp.sum(jnp.where(hits, lists % per_block, 0), -1)
    asked = jnp.any(hits, -1)
    outbound = pl.pallas_call(
        outbound_kernel,
        out_shape=jax.ShapeDtypeStruct((owners, ROWS, 2 * DH), LOW),
        in_specs=[smem(), vmem(), vmem()],
        out_specs=vmem(),
        scratch_shapes=[pltpu.VMEM((per_block, BLK, 2 * DH), LOW)],
        name="outbound",
    )(wanted, keys, values)
    arrived = lax.all_to_all(outbound, KV, split_axis=0, concat_axis=0, tiled=True)

    gated = gates[..., None] * cotangent.reshape(rows, heads, DH).astype(WIDE)[None]
    delta = jnp.sum(gated * branch_out.reshape(2, rows, heads, DH).astype(WIDE), -1)
    ld = jnp.stack([log_sums, delta], -1)
    gated_low = gated.astype(LOW)
    zero = jnp.zeros((rows, heads, DH), LOW)
    q_part = jnp.concatenate([queries.reshape(rows, heads, DH) * LOW(DH ** (-0.5)), zero], -1)
    g_part = [jnp.concatenate([zero, gated_low[b]], -1) for b in range(2)]
    m_sum = jnp.transpose(jnp.stack([q_part, g_part[0]]), (0, 2, 1, 3)).reshape(-1, 2 * DH)
    m_sel = jnp.stack([q_part, g_part[1]]).reshape(2, SUB, sub_rows, heads, 2 * DH)
    m_sel = jnp.transpose(m_sel, (1, 0, 3, 2, 4)).reshape(SUB, -1, 2 * DH)
    ld_sum = jnp.transpose(ld[0], (1, 0, 2)).reshape(-1, 2)
    ld_sel = jnp.transpose(ld[1].reshape(SUB, sub_rows, heads, 2), (0, 2, 1, 3)).reshape(SUB, -1, 2)
    listing = lax.dynamic_index_in_dim(lists, place, 0, keepdims=False)
    live = listing >= 0
    own = jnp.where(live, listing // per_block, -1)
    starts = jnp.where(live, listing * BLK - place * rows, FAR)
    rel_sel = (starts[:, None] + jnp.arange(BLK, dtype=jnp.int32)).reshape(SUB, TOPN * BLK)
    slot = jnp.arange(owners * (ROWS - BLK), dtype=jnp.int32)
    inner = slot % (ROWS - BLK)
    ends = (slot // (ROWS - BLK) * per_block + inner + 1) * CMP - 1 - place * rows
    rel_sum = jnp.where(inner < per_block, ends, FAR)[None]

    grad_queries, returned = pl.pallas_call(
        main_kernel,
        out_shape=(
            jax.ShapeDtypeStruct((rows, heads * DH), WIDE),
            jax.ShapeDtypeStruct((owners, ROWS, 2 * DH), LOW),
        ),
        in_specs=[smem()] + [vmem()] * 7,
        out_specs=(vmem(), vmem()),
        scratch_shapes=[pltpu.VMEM((TOPN * BLK, 2 * DH), LOW)],
        name="main",
    )(own, m_sum, m_sel, ld_sum, ld_sel, rel_sum, rel_sel, arrived)
    incoming = lax.all_to_all(returned, KV, split_axis=0, concat_axis=0, tiled=True)

    parts = pl.pallas_call(
        weight_kernel,
        out_shape=jax.ShapeDtypeStruct((fast, hidden.shape[1] // fast, heads * DH), LOW),
        in_specs=[vmem(), vmem()],
        out_specs=vmem(),
        name="weight",
    )(hidden, grad_queries)
    across = lax.all_to_all(parts, KV[1], split_axis=0, concat_axis=0, tiled=True)
    column = jnp.sum(across.astype(WIDE), 0).astype(LOW).reshape(slow, -1, heads * DH)
    along = lax.all_to_all(column, KV[0], split_axis=0, concat_axis=0, tiled=True)
    grad_weight = jnp.sum(along.astype(WIDE), 0)

    grad_keys, grad_values = pl.pallas_call(
        inbound_kernel,
        out_shape=(jax.ShapeDtypeStruct((rows, DH), WIDE), jax.ShapeDtypeStruct((rows, DH), WIDE)),
        in_specs=[smem(), vmem()],
        out_specs=(vmem(), vmem()),
        name="inbound",
    )(jnp.where(asked, wanted, per_block), incoming)
    return (grad_queries, grad_keys, grad_values, grad_weight)


def solution(mesh):
    finer = Mesh(mesh.devices.reshape(16, 8, mesh.shape["tp"]), ("kv_0", "kv_1", "tp"))
    placed = (
        P(KV, "tp"),
        P(KV, "tp"),
        P(KV, "tp"),
        P(KV, None),
        P(None, KV, "tp"),
        P(None, KV, "tp"),
        P(None, KV, "tp"),
        P(KV, "tp"),
        P(None, "tp", None),
    )
    return jax.shard_map(
        shards,
        mesh=finer,
        in_specs=placed,
        out_specs=(P(KV, "tp"), P(KV, "tp"), P(KV, "tp"), P(KV, "tp")),
        check_vma=False,
    )
```

```python
import jax
import jax.numpy as jnp
from jax import lax
from jax.experimental import pallas as pl
from jax.experimental.pallas import tpu as pltpu
from jax.sharding import Mesh
from jax.sharding import PartitionSpec as P

DH = 64
BLK = 32
TOPN = 12
SUB = 4
CMP = 32
KV = ("kv_0", "kv_1")
FAR = 1 << 30
WIDE = jnp.float32
LOW = jnp.bfloat16
SLOW = 16
FAST = 8
PER = 4
PAIR = 2 * DH
ROWS = PER * BLK
SUB_ROWS = ROWS // SUB
COLS = 16
FETCH = SLOW * (BLK + PER)
SUMS = SLOW * BLK
PARTS = SLOW * (BLK + PER)
BACK = PARTS + SLOW * COLS
LAST = ROWS + 8 + COLS


def dot(a, b, ca, cb):
    return lax.dot_general(a, b, (((ca,), (cb,)), ((), ())), preferred_element_type=WIDE)


def pairs_kernel(keys_ref, values_ref, out_ref):
    both = jnp.concatenate([keys_ref[...], values_ref[...]], 0).astype(WIDE)
    out_ref[...] = both.T.astype(LOW)


def relay_kernel(table_ref, all_ref, out_ref):
    rows = all_ref[...].astype(WIDE).reshape(SLOW * PER, CMP, PAIR)
    means = jnp.mean(rows, 1).astype(LOW)
    for y in range(FAST):
        out_ref[y, SUMS:, :] = means

    def one(z, carry):
        for y in range(FAST):
            at = (z * PER + jnp.minimum(table_ref[y * SLOW + z], PER - 1)) * BLK
            out_ref[y, pl.ds(pl.multiple_of(z * BLK, BLK), BLK), :] = all_ref[
                pl.ds(pl.multiple_of(at, BLK), BLK), :
            ]
        return carry

    lax.fori_loop(0, SLOW, one, 0)


def prep_kernel(q_ref, cot_ref, gates_ref, logs_ref, out_ref, msum_ref, msel_ref, ldsum_ref, ldsel_ref):
    cols = jnp.concatenate([gates_ref[0], gates_ref[1], logs_ref[0], logs_ref[1]], 0).T
    first = lax.broadcasted_iota(jnp.int32, (ROWS, PAIR), 1) < DH
    q = q_ref[...].astype(WIDE) * (DH ** (-0.5))
    heads_q = [jnp.where(first, q, 0.0).astype(LOW), jnp.where(first, pltpu.roll(q, DH, 1), 0.0).astype(LOW)]
    cot = cot_ref[...].astype(WIDE)
    for b in range(2):
        g = jnp.where(first, cols[:, 2 * b:2 * b + 1], cols[:, 2 * b + 1:2 * b + 2]) * cot
        terms = g * out_ref[b].astype(WIDE)
        heads_g = [jnp.where(first, 0.0, pltpu.roll(g, DH, 1)).astype(LOW), jnp.where(first, 0.0, g).astype(LOW)]
        deltas = [
            jnp.sum(jnp.where(first, terms, 0.0), -1, keepdims=True),
            jnp.sum(jnp.where(first, 0.0, terms), -1, keepdims=True),
        ]
        for h in range(2):
            ld = jnp.concatenate([cols[:, 4 + 2 * b + h:5 + 2 * b + h], deltas[h]], 1)
            if b == 0:
                msum_ref[h * ROWS:(h + 1) * ROWS, :] = heads_q[h]
                msum_ref[(2 + h) * ROWS:(3 + h) * ROWS, :] = heads_g[h]
                ldsum_ref[h * ROWS:(h + 1) * ROWS, :] = ld
            else:
                for s in range(SUB):
                    here = slice(s * SUB_ROWS, (s + 1) * SUB_ROWS)
                    msel_ref[s, h * SUB_ROWS:(h + 1) * SUB_ROWS, :] = heads_q[h][here]
                    msel_ref[s, (2 + h) * SUB_ROWS:(3 + h) * SUB_ROWS, :] = heads_g[h][here]
                    ldsel_ref[s, h * SUB_ROWS:(h + 1) * SUB_ROWS, :] = ld[here]


def main_kernel(place_ref, list_ref, msum_ref, msel_ref, ldsum_ref, ldsel_ref, arr_ref, hid_ref,
                dq_ref, ret_ref, kv_ref, hid_here, sem):
    load = pltpu.make_async_copy(hid_ref, hid_here, sem)
    load.start()
    base = place_ref[0] * ROWS
    scale = DH ** (-0.5)

    def grads(m, kv, seen, ld):
        half = m.shape[0] // 2
        sd = dot(m, kv, 1, 1)
        probs = jnp.where(seen, jnp.exp(sd[:half] - ld[:, :1]), 0.0)
        ds = (probs * (sd[half:] - ld[:, 1:2])).astype(LOW)
        weights = jnp.concatenate([ds, probs.astype(LOW)], 0)
        return dot(ds, kv, 1, 0), dot(weights, m, 0, 0)

    m = msum_ref[...]
    ld = ldsum_ref[...]
    row_at = lax.broadcasted_iota(jnp.int32, (2 * ROWS, 1), 0) & (ROWS - 1)
    per_fast = SLOW * PER
    step = 4
    lane = lax.broadcasted_iota(jnp.int32, (1, step * per_fast), 1)
    dq_sum = jnp.zeros((2 * ROWS, PAIR), WIDE)
    for y in range(0, FAST, step):
        kv = jnp.concatenate([arr_ref[y + k, SUMS:, :] for k in range(step)], 0)
        owner = (lane & (per_fast - 1)) // PER * FAST + y + lane // per_fast
        ends = (owner * PER + (lane & (PER - 1)) + 1) * CMP - 1 - base
        dq_part, kv_grad = grads(m, kv, ends <= row_at, ld)
        dq_sum += dq_part
        low = kv_grad.astype(LOW)
        for k in range(step):
            ret_ref[y + k, SUMS:PARTS, :] = low[k * per_fast:(k + 1) * per_fast]
    sub_at = lax.broadcasted_iota(jnp.int32, (2 * SUB_ROWS, 1), 0) & (SUB_ROWS - 1)
    sel_lane = lax.broadcasted_iota(jnp.int32, (1, TOPN * BLK), 1)
    for s in range(SUB):
        at_key = jnp.full((1, TOPN * BLK), FAR, jnp.int32)
        places = []
        for i in range(TOPN):
            n = list_ref[s * TOPN + i]
            live = n >= 0
            owner = jnp.maximum(n, 0) // PER
            fast = owner & (FAST - 1)
            at = pl.multiple_of(owner // FAST * BLK, BLK)
            places.append((live, fast, at))
            kv_ref[i * BLK:(i + 1) * BLK, :] = arr_ref[fast, pl.ds(at, BLK), :]
            start = jnp.where(live, n * BLK - base - i * BLK, FAR)
            at_key = jnp.where(sel_lane // BLK == i, start, at_key)
        kv = kv_ref[...]
        seen = at_key + sel_lane <= sub_at + s * SUB_ROWS
        dq_part, kv_grad = grads(msel_ref[s], kv, seen, ldsel_ref[s])
        low = kv_grad.astype(LOW)
        for i in range(TOPN):
            live, fast, at = places[i]

            @pl.when(live)
            def _(fast=fast, at=at, i=i):
                ret_ref[fast, pl.ds(at, BLK), :] = low[i * BLK:(i + 1) * BLK]

        top = s * SUB_ROWS
        for h in range(2):
            total = dq_sum[h * ROWS + top:h * ROWS + top + SUB_ROWS, :DH]
            total = total + dq_part[h * SUB_ROWS:(h + 1) * SUB_ROWS, :DH]
            dq_ref[top:top + SUB_ROWS, h * DH:(h + 1) * DH] = total * scale
    load.wait()
    qb = dq_ref[...].astype(LOW)
    span = FAST * COLS
    for z in range(SLOW):
        part = dot(hid_here[:, z * span:(z + 1) * span], qb, 0, 0).astype(LOW)
        for y in range(FAST):
            ret_ref[y, PARTS + z * COLS:PARTS + (z + 1) * COLS, :] = part[y * COLS:(y + 1) * COLS]


def merge_kernel(table_ref, in_ref, out_ref, tail_ref):
    tail = in_ref[0, SUMS:PARTS, :].astype(WIDE)
    for y in range(1, FAST):
        tail = tail + in_ref[y, SUMS:PARTS, :].astype(WIDE)
    tail_ref[:SLOW * PER, :] = tail
    tail_ref[SLOW * PER:, :] = jnp.zeros((8, PAIR), WIDE)

    def one(z, carry):
        sums = [jnp.zeros((BLK, PAIR), WIDE) for _ in range(PER)]
        cols = jnp.zeros((COLS, PAIR), WIDE)
        for y in range(FAST):
            pick = table_ref[y * SLOW + z]
            here = in_ref[y, pl.ds(pl.multiple_of(z * BLK, BLK), BLK), :].astype(WIDE)
            sums = [sums[b] + jnp.where(pick == b, here, 0.0) for b in range(PER)]
            cols = cols + in_ref[y, pl.ds(pl.multiple_of(PARTS + z * COLS, COLS), COLS), :].astype(WIDE)
        for b in range(PER):
            out_ref[z, b * BLK:(b + 1) * BLK, :] = sums[b].astype(LOW)
        out_ref[z, ROWS:ROWS + 8, :] = tail_ref[pl.ds(z * PER, 8), :].astype(LOW)
        out_ref[z, ROWS + 8:, :] = cols.astype(LOW)
        return carry

    lax.fori_loop(0, SLOW, one, 0)


def final_kernel(in_ref, gk_ref, gv_ref, gw_ref):
    total = in_ref[0].astype(WIDE)
    for z in range(1, SLOW):
        total = total + in_ref[z].astype(WIDE)
    rows = [
        total[b * BLK:(b + 1) * BLK] + total[ROWS + b:ROWS + b + 1] * (1.0 / CMP) for b in range(PER)
    ]
    turned = jnp.concatenate(rows, 0).T
    gk_ref[...] = turned[:DH]
    gv_ref[...] = turned[DH:]
    gw_ref[...] = total[ROWS + 8:]


def vmem():
    return pl.BlockSpec(memory_space=pltpu.VMEM)


def smem():
    return pl.BlockSpec(memory_space=pltpu.SMEM)


def shape(*sizes, kind=LOW):
    return jax.ShapeDtypeStruct(sizes, kind)


def call(kernel, ins, outs, scratch=()):
    many = isinstance(outs, tuple)
    return pl.pallas_call(
        kernel,
        out_shape=outs,
        in_specs=ins,
        out_specs=tuple(vmem() for _ in outs) if many else vmem(),
        scratch_shapes=list(scratch),
        name=kernel.__name__,
    )


def shards(queries, keys, values, hidden, log_sums, gates, branch_out, cotangent, chosen):
    slow_at = lax.axis_index(KV[0])
    fast_at = lax.axis_index(KV[1])
    place = slow_at * FAST + fast_at
    lists = chosen[:, 0]
    near = lax.dynamic_slice_in_dim(lists, slow_at * FAST, FAST, 0)
    owner = near // PER
    ours = (near >= 0) & (owner % FAST == fast_at)
    hits = ours[..., None] & ((owner // FAST)[..., None] == jnp.arange(SLOW, dtype=jnp.int32))
    table = jnp.min(jnp.where(hits, (near % PER)[..., None], PER), 1).reshape(-1)
    listing = lax.dynamic_index_in_dim(lists, place, 0, keepdims=False)

    pairs = call(pairs_kernel, [vmem(), vmem()], shape(ROWS, PAIR))(keys.T, values.T)
    along = lax.all_gather(pairs, KV[0], axis=0, tiled=True)
    outbound = call(relay_kernel, [smem(), vmem()], shape(FAST, FETCH, PAIR))(table, along)
    arrived = lax.all_to_all(outbound, KV[1], split_axis=0, concat_axis=0, tiled=True)

    m_sum, m_sel, ld_sum, ld_sel = call(
        prep_kernel,
        [vmem()] * 5,
        (
            shape(4 * ROWS, PAIR),
            shape(SUB, 4 * SUB_ROWS, PAIR),
            shape(2 * ROWS, 2, kind=WIDE),
            shape(SUB, 2 * SUB_ROWS, 2, kind=WIDE),
        ),
    )(queries, cotangent, jnp.transpose(gates, (0, 2, 1)), jnp.transpose(log_sums, (0, 2, 1)), branch_out)
    grad_queries, returned = call(
        main_kernel,
        [smem(), smem()] + [vmem()] * 5 + [pl.BlockSpec(memory_space=pl.ANY)],
        (shape(ROWS, PAIR, kind=WIDE), shape(FAST, BACK, PAIR)),
        (
            pltpu.VMEM((TOPN * BLK, PAIR), LOW),
            pltpu.VMEM(hidden.shape, LOW),
            pltpu.SemaphoreType.DMA,
        ),
    )(place[None], listing, m_sum, m_sel, ld_sum, ld_sel, arrived, hidden)
    across = lax.all_to_all(returned, KV[1], split_axis=0, concat_axis=0, tiled=True)
    merged = call(
        merge_kernel,
        [smem(), vmem()],
        shape(SLOW, LAST, PAIR),
        (pltpu.VMEM((SLOW * PER + 8, PAIR), WIDE),),
    )(table, across)
    home = lax.all_to_all(merged, KV[0], split_axis=0, concat_axis=0, tiled=True)
    turned_keys, turned_values, grad_weight = call(
        final_kernel,
        [vmem()],
        (shape(DH, ROWS, kind=WIDE), shape(DH, ROWS, kind=WIDE), shape(COLS, PAIR, kind=WIDE)),
    )(home)
    return (grad_queries, turned_keys.T, turned_values.T, grad_weight)


def solution(mesh):
    finer = Mesh(mesh.devices.reshape(SLOW, FAST, mesh.shape["tp"]), ("kv_0", "kv_1", "tp"))
    placed = (
        P(KV, "tp"),
        P(KV, "tp"),
        P(KV, "tp"),
        P(KV, None),
        P(None, KV, "tp"),
        P(None, KV, "tp"),
        P(None, KV, "tp"),
        P(KV, "tp"),
        P(None, "tp", None),
    )
    return jax.shard_map(
        shards,
        mesh=finer,
        in_specs=placed,
        out_specs=(P(KV, "tp"), P(KV, "tp"), P(KV, "tp"), P(KV, "tp")),
        check_vma=False,
    )
```

```python
import jax
import jax.numpy as jnp
from jax import lax
from jax.experimental import pallas as pl
from jax.experimental.pallas import tpu as pltpu
from jax.sharding import Mesh
from jax.sharding import PartitionSpec as P

DH = 64
BLK = 32
TOPN = 12
SUB = 4
CMP = 32
KV = ("kv_0", "kv_1")
FAR = 1 << 30
WIDE = jnp.float32
LOW = jnp.bfloat16
SLOW = 16
FAST = 8
PER = 4
PAIR = 2 * DH
ROWS = PER * BLK
SUB_ROWS = ROWS // SUB
COLS = 16
FETCH = SLOW * (BLK + PER)
SUMS = SLOW * BLK
PARTS = SLOW * (BLK + PER)
BACK = PARTS + SLOW * COLS
LAST = ROWS + 8 + COLS


def dot(a, b, ca, cb):
    return lax.dot_general(a, b, (((ca,), (cb,)), ((), ())), preferred_element_type=WIDE)


def pairs_kernel(place_ref, keys_ref, values_ref, chosen_ref, out_ref, table_ref):
    both = jnp.concatenate([keys_ref[...], values_ref[...]], 0).astype(WIDE)
    out_ref[...] = both.T.astype(LOW)
    entry = chosen_ref[...]
    fast_at = place_ref[0] & (FAST - 1)
    owner = jnp.where(entry >= 0, entry // PER, -1)
    inner = entry & (PER - 1)
    for z in range(SLOW):
        hit = jnp.where(owner == z * FAST + fast_at, inner, PER)
        table_ref[z:z + 1, :] = jnp.min(hit, 0, keepdims=True)


def relay_kernel(place_ref, table_ref, all_ref, out_ref, mean_ref):
    step = pl.program_id(0)
    per_step = out_ref.shape[0]
    column = place_ref[0] // FAST * FAST

    @pl.when(step == 0)
    def _():
        rows = all_ref[...].astype(WIDE).reshape(SLOW * PER, CMP, PAIR)
        mean_ref[...] = jnp.mean(rows, 1).astype(LOW)

    for k in range(per_step):
        out_ref[k, SUMS:, :] = mean_ref[...]

        def one(z, carry, k=k):
            pick = jnp.minimum(table_ref[z, column + step * per_step + k], PER - 1)
            at = pl.multiple_of((z * PER + pick) * BLK, BLK)
            out_ref[k, pl.ds(pl.multiple_of(z * BLK, BLK), BLK), :] = all_ref[pl.ds(at, BLK), :]
            return carry

        lax.fori_loop(0, SLOW, one, 0, unroll=4)


def prep_kernel(q_ref, cot_ref, gates_ref, logs_ref, out_ref, msum_ref, msel_ref, ldsum_ref, ldsel_ref):
    cols = jnp.concatenate([gates_ref[0], gates_ref[1], logs_ref[0], logs_ref[1]], 0).T
    first = lax.broadcasted_iota(jnp.int32, (ROWS, PAIR), 1) < DH
    q = q_ref[...].astype(WIDE) * (DH ** (-0.5))
    heads_q = [jnp.where(first, q, 0.0).astype(LOW), jnp.where(first, pltpu.roll(q, DH, 1), 0.0).astype(LOW)]
    cot = cot_ref[...].astype(WIDE)
    for b in range(2):
        g = jnp.where(first, cols[:, 2 * b:2 * b + 1], cols[:, 2 * b + 1:2 * b + 2]) * cot
        terms = g * out_ref[b].astype(WIDE)
        heads_g = [jnp.where(first, 0.0, pltpu.roll(g, DH, 1)).astype(LOW), jnp.where(first, 0.0, g).astype(LOW)]
        deltas = [
            jnp.sum(jnp.where(first, terms, 0.0), -1, keepdims=True),
            jnp.sum(jnp.where(first, 0.0, terms), -1, keepdims=True),
        ]
        for h in range(2):
            ld = jnp.concatenate([cols[:, 4 + 2 * b + h:5 + 2 * b + h], deltas[h]], 1)
            if b == 0:
                msum_ref[h * ROWS:(h + 1) * ROWS, :] = heads_q[h]
                msum_ref[(2 + h) * ROWS:(3 + h) * ROWS, :] = heads_g[h]
                ldsum_ref[h * ROWS:(h + 1) * ROWS, :] = ld
            else:
                for s in range(SUB):
                    here = slice(s * SUB_ROWS, (s + 1) * SUB_ROWS)
                    msel_ref[s, h * SUB_ROWS:(h + 1) * SUB_ROWS, :] = heads_q[h][here]
                    msel_ref[s, (2 + h) * SUB_ROWS:(3 + h) * SUB_ROWS, :] = heads_g[h][here]
                    ldsel_ref[s, h * SUB_ROWS:(h + 1) * SUB_ROWS, :] = ld[here]


def main_kernel(place_ref, list_ref, msum_ref, msel_ref, ldsum_ref, ldsel_ref, arr_ref, hid_ref,
                dq_ref, out_ref, kv_ref, hid_here, arr_here, ret_ref, sems):
    load_sums = pltpu.make_async_copy(arr_ref.at[:, SUMS:], arr_here.at[:, SUMS:], sems.at[0])
    load_sums.start()
    load_blocks = pltpu.make_async_copy(arr_ref.at[:, :SUMS], arr_here.at[:, :SUMS], sems.at[1])
    load_blocks.start()
    load_hidden = pltpu.make_async_copy(hid_ref, hid_here, sems.at[2])
    load_hidden.start()
    base = place_ref[0] * ROWS
    scale = DH ** (-0.5)

    def grads(m, kv, seen, ld):
        half = m.shape[0] // 2
        sd = dot(m, kv, 1, 1)
        probs = jnp.where(seen, jnp.exp(sd[:half] - ld[:, :1]), 0.0)
        ds = (probs * (sd[half:] - ld[:, 1:2])).astype(LOW)
        weights = jnp.concatenate([ds, probs.astype(LOW)], 0)
        return dot(ds, kv, 1, 0), dot(weights, m, 0, 0)

    m = msum_ref[...]
    ld = ldsum_ref[...]
    row_at = lax.broadcasted_iota(jnp.int32, (2 * ROWS, 1), 0) & (ROWS - 1)
    per_fast = SLOW * PER
    step = 4
    lane = lax.broadcasted_iota(jnp.int32, (1, step * per_fast), 1)
    dq_sum = jnp.zeros((2 * ROWS, PAIR), WIDE)
    load_sums.wait()
    for y in range(0, FAST, step):
        kv = jnp.concatenate([arr_here[y + k, SUMS:, :] for k in range(step)], 0)
        owner = (lane & (per_fast - 1)) // PER * FAST + y + lane // per_fast
        ends = (owner * PER + (lane & (PER - 1)) + 1) * CMP - 1 - base
        dq_part, kv_grad = grads(m, kv, ends <= row_at, ld)
        dq_sum += dq_part
        low = kv_grad.astype(LOW)
        for k in range(step):
            ret_ref[y + k, SUMS:PARTS, :] = low[k * per_fast:(k + 1) * per_fast]
    load_blocks.wait()
    sub_at = lax.broadcasted_iota(jnp.int32, (2 * SUB_ROWS, 1), 0) & (SUB_ROWS - 1)
    sel_lane = lax.broadcasted_iota(jnp.int32, (1, TOPN * BLK), 1)
    for s in range(SUB):
        at_key = jnp.full((1, TOPN * BLK), FAR, jnp.int32)
        places = []
        for i in range(TOPN):
            n = list_ref[s * TOPN + i]
            live = n >= 0
            owner = jnp.maximum(n, 0) // PER
            fast = owner & (FAST - 1)
            at = pl.multiple_of(owner // FAST * BLK, BLK)
            places.append((live, fast, at))
            kv_ref[i * BLK:(i + 1) * BLK, :] = arr_here[fast, pl.ds(at, BLK), :]
            start = jnp.where(live, n * BLK - base - i * BLK, FAR)
            at_key = jnp.where(sel_lane // BLK == i, start, at_key)
        kv = kv_ref[...]
        seen = at_key + sel_lane <= sub_at + s * SUB_ROWS
        dq_part, kv_grad = grads(msel_ref[s], kv, seen, ldsel_ref[s])
        low = kv_grad.astype(LOW)
        for i in range(TOPN):
            live, fast, at = places[i]

            @pl.when(live)
            def _(fast=fast, at=at, i=i):
                ret_ref[fast, pl.ds(at, BLK), :] = low[i * BLK:(i + 1) * BLK]

        top = s * SUB_ROWS
        for h in range(2):
            total = dq_sum[h * ROWS + top:h * ROWS + top + SUB_ROWS, :DH]
            total = total + dq_part[h * SUB_ROWS:(h + 1) * SUB_ROWS, :DH]
            dq_ref[top:top + SUB_ROWS, h * DH:(h + 1) * DH] = total * scale
    store_first = pltpu.make_async_copy(ret_ref.at[:, :PARTS], out_ref.at[:, :PARTS], sems.at[3])
    store_first.start()
    load_hidden.wait()
    qb = dq_ref[...].astype(LOW)
    span = FAST * COLS
    for z in range(SLOW):
        part = dot(hid_here[:, z * span:(z + 1) * span], qb, 0, 0).astype(LOW)
        for y in range(FAST):
            ret_ref[y, PARTS + z * COLS:PARTS + (z + 1) * COLS, :] = part[y * COLS:(y + 1) * COLS]
    store_rest = pltpu.make_async_copy(ret_ref.at[:, PARTS:], out_ref.at[:, PARTS:], sems.at[4])
    store_rest.start()
    store_first.wait()
    store_rest.wait()


def merge_kernel(place_ref, table_ref, in_ref, sums_ref, parts_ref, out_ref, tail_ref):
    step = pl.program_id(0)
    per_step = out_ref.shape[0]
    column = place_ref[0] // FAST * FAST

    @pl.when(step == 0)
    def _():
        tail = sums_ref[0].astype(WIDE)
        for y in range(1, FAST):
            tail = tail + sums_ref[y].astype(WIDE)
        tail_ref[:SLOW * PER, :] = tail
        tail_ref[SLOW * PER:, :] = jnp.zeros((8, PAIR), WIDE)

    def one(k, carry):
        z = step * per_step + k
        sums = [jnp.zeros((BLK, PAIR), WIDE) for _ in range(PER)]
        cols = jnp.zeros((COLS, PAIR), WIDE)
        for y in range(FAST):
            pick = table_ref[z, column + y]
            here = in_ref[y, pl.ds(pl.multiple_of(k * BLK, BLK), BLK), :].astype(WIDE)
            sums = [sums[b] + jnp.where(pick == b, here, 0.0) for b in range(PER)]
            cols = cols + parts_ref[y, pl.ds(pl.multiple_of(k * COLS, COLS), COLS), :].astype(WIDE)
        for b in range(PER):
            out_ref[k, b * BLK:(b + 1) * BLK, :] = sums[b].astype(LOW)
        out_ref[k, ROWS:ROWS + 8, :] = tail_ref[pl.ds(z * PER, 8), :].astype(LOW)
        out_ref[k, ROWS + 8:, :] = cols.astype(LOW)
        return carry

    lax.fori_loop(0, per_step, one, 0)


def final_kernel(in_ref, gk_ref, gv_ref, gw_ref, total_ref):
    step = pl.program_id(0)
    part = in_ref[0].astype(WIDE)
    for z in range(1, in_ref.shape[0]):
        part = part + in_ref[z].astype(WIDE)

    @pl.when(step == 0)
    def _():
        total_ref[...] = part

    @pl.when(step > 0)
    def _():
        total_ref[...] += part

    @pl.when(step == pl.num_programs(0) - 1)
    def _():
        total = total_ref[...]
        rows = [
            total[b * BLK:(b + 1) * BLK] + total[ROWS + b:ROWS + b + 1] * (1.0 / CMP) for b in range(PER)
        ]
        turned = jnp.concatenate(rows, 0).T
        gk_ref[...] = turned[:DH]
        gv_ref[...] = turned[DH:]
        gw_ref[...] = total[ROWS + 8:]


def vmem():
    return pl.BlockSpec(memory_space=pltpu.VMEM)


def smem():
    return pl.BlockSpec(memory_space=pltpu.SMEM)


def shape(*sizes, kind=LOW):
    return jax.ShapeDtypeStruct(sizes, kind)


def piece(sizes, at):
    return pl.BlockSpec(sizes, at)


def call(kernel, ins, outs, specs, scratch=(), grid=()):
    return pl.pallas_call(
        kernel,
        grid=grid,
        out_shape=outs,
        in_specs=ins,
        out_specs=specs,
        scratch_shapes=list(scratch),
        name=kernel.__name__,
    )


def shards(queries, keys, values, hidden, log_sums, gates, branch_out, cotangent, chosen):
    place = lax.axis_index(KV)
    here = place[None]
    lists = chosen[:, 0]
    pairs, table = call(
        pairs_kernel,
        [smem(), vmem(), vmem(), vmem()],
        (shape(ROWS, PAIR), shape(SLOW, lists.shape[0], kind=jnp.int32)),
        (vmem(), vmem()),
    )(here, keys.T, values.T, lists.T)
    along = lax.all_gather(pairs, KV[0], axis=0, tiled=True)
    outbound = call(
        relay_kernel,
        [smem(), smem(), piece((SLOW * ROWS, PAIR), lambda i: (0, 0))],
        shape(FAST, FETCH, PAIR),
        piece((FAST // 4, FETCH, PAIR), lambda i: (i, 0, 0)),
        (pltpu.VMEM((SLOW * PER, PAIR), LOW),),
        grid=(4,),
    )(here, table, along)
    arrived = lax.all_to_all(outbound, KV[1], split_axis=0, concat_axis=0, tiled=True)

    listing = lax.dynamic_index_in_dim(lists, place, 0, keepdims=False)
    m_sum, m_sel, ld_sum, ld_sel = call(
        prep_kernel,
        [vmem()] * 5,
        (
            shape(4 * ROWS, PAIR),
            shape(SUB, 4 * SUB_ROWS, PAIR),
            shape(2 * ROWS, 2, kind=WIDE),
            shape(SUB, 2 * SUB_ROWS, 2, kind=WIDE),
        ),
        (vmem(),) * 4,
    )(queries, cotangent, jnp.transpose(gates, (0, 2, 1)), jnp.transpose(log_sums, (0, 2, 1)), branch_out)
    grad_queries, returned = call(
        main_kernel,
        [smem(), smem()] + [vmem()] * 4 + [pl.BlockSpec(memory_space=pl.ANY)] * 2,
        (shape(ROWS, PAIR, kind=WIDE), shape(FAST, BACK, PAIR)),
        (vmem(), pl.BlockSpec(memory_space=pl.ANY)),
        (
            pltpu.VMEM((TOPN * BLK, PAIR), LOW),
            pltpu.VMEM(hidden.shape, LOW),
            pltpu.VMEM((FAST, FETCH, PAIR), LOW),
            pltpu.VMEM((FAST, BACK, PAIR), LOW),
            pltpu.SemaphoreType.DMA((5,)),
        ),
    )(here, listing, m_sum, m_sel, ld_sum, ld_sel, arrived, hidden)
    across = lax.all_to_all(returned, KV[1], split_axis=0, concat_axis=0, tiled=True)
    per_step = SLOW // 4
    merged = call(
        merge_kernel,
        [
            smem(),
            smem(),
            piece((FAST, per_step * BLK, PAIR), lambda i: (0, i, 0)),
            piece((FAST, SLOW * PER, PAIR), lambda i: (0, SUMS // (SLOW * PER), 0)),
            piece((FAST, per_step * COLS, PAIR), lambda i: (0, PARTS // (per_step * COLS) + i, 0)),
        ],
        shape(SLOW, LAST, PAIR),
        piece((per_step, LAST, PAIR), lambda i: (i, 0, 0)),
        (pltpu.VMEM((SLOW * PER + 8, PAIR), WIDE),),
        grid=(4,),
    )(here, table, across, across, across)
    home = lax.all_to_all(merged, KV[0], split_axis=0, concat_axis=0, tiled=True)
    whole = lambda i: (0, 0)
    turned_keys, turned_values, grad_weight = call(
        final_kernel,
        [piece((SLOW // 4, LAST, PAIR), lambda i: (i, 0, 0))],
        (shape(DH, ROWS, kind=WIDE), shape(DH, ROWS, kind=WIDE), shape(COLS, PAIR, kind=WIDE)),
        (piece((DH, ROWS), whole), piece((DH, ROWS), whole), piece((COLS, PAIR), whole)),
        (pltpu.VMEM((LAST, PAIR), WIDE),),
        grid=(4,),
    )(home)
    return (grad_queries, turned_keys.T, turned_values.T, grad_weight)


def solution(mesh):
    finer = Mesh(mesh.devices.reshape(SLOW, FAST, mesh.shape["tp"]), ("kv_0", "kv_1", "tp"))
    placed = (
        P(KV, "tp"),
        P(KV, "tp"),
        P(KV, "tp"),
        P(KV, None),
        P(None, KV, "tp"),
        P(None, KV, "tp"),
        P(None, KV, "tp"),
        P(KV, "tp"),
        P(None, "tp", None),
    )
    return jax.shard_map(
        shards,
        mesh=finer,
        in_specs=placed,
        out_specs=(P(KV, "tp"), P(KV, "tp"), P(KV, "tp"), P(KV, "tp")),
        check_vma=False,
    )
```

```python
import jax
import jax.numpy as jnp
from jax import lax
from jax.experimental import pallas as pl
from jax.experimental.pallas import tpu as pltpu
from jax.sharding import Mesh
from jax.sharding import PartitionSpec as P

DH = 64
BLK = 32
TOPN = 12
SUB = 4
CMP = 32
KV = ("kv_0", "kv_1", "kv_2")
GROUP_AXES = KV[1:]
FAR = 1 << 30
WIDE = jnp.float32
LOW = jnp.bfloat16
NEAR = 4
SLOW = 16 // NEAR
GROUP = 8 * NEAR
PER = 4
PAIR = 2 * DH
ROWS = PER * BLK
SUB_ROWS = ROWS // SUB
COLS = 16
FETCH = SLOW * (BLK + PER)
SUMS = SLOW * BLK
PARTS = SLOW * (BLK + PER)
BACK = PARTS + SLOW * COLS
LAST = ROWS + 8 + COLS


def dot(a, b, ca, cb):
    return lax.dot_general(a, b, (((ca,), (cb,)), ((), ())), preferred_element_type=WIDE)


def pairs_kernel(place_ref, keys_ref, values_ref, chosen_ref, out_ref, table_ref):
    both = jnp.concatenate([keys_ref[...], values_ref[...]], 0).astype(WIDE)
    out_ref[...] = both.T.astype(LOW)
    entry = chosen_ref[...]
    own = place_ref[0] & (GROUP - 1)
    owner = jnp.where(entry >= 0, entry // PER, -1)
    inner = entry & (PER - 1)
    for z in range(SLOW):
        hit = jnp.where(owner == z * GROUP + own, inner, PER)
        table_ref[z:z + 1, :] = jnp.min(hit, 0, keepdims=True)


def relay_kernel(place_ref, table_ref, all_ref, out_ref):
    column = place_ref[0] // GROUP * GROUP
    rows = all_ref[...].astype(WIDE).reshape(SLOW * PER, CMP, PAIR)
    means = jnp.mean(rows, 1).astype(LOW)

    def one(g, carry):
        out_ref[g, SUMS:, :] = means
        for z in range(SLOW):
            pick = jnp.minimum(table_ref[z, column + g], PER - 1)
            at = pl.multiple_of((z * PER + pick) * BLK, BLK)
            out_ref[g, z * BLK:(z + 1) * BLK, :] = all_ref[pl.ds(at, BLK), :]
        return carry

    lax.fori_loop(0, GROUP, one, 0, unroll=2)


def prep_kernel(q_ref, cot_ref, gates_ref, logs_ref, out_ref, msum_ref, msel_ref, ldsum_ref, ldsel_ref):
    cols = jnp.concatenate([gates_ref[0], gates_ref[1], logs_ref[0], logs_ref[1]], 0).T
    first = lax.broadcasted_iota(jnp.int32, (ROWS, PAIR), 1) < DH
    q = q_ref[...].astype(WIDE) * (DH ** (-0.5))
    heads_q = [jnp.where(first, q, 0.0).astype(LOW), jnp.where(first, pltpu.roll(q, DH, 1), 0.0).astype(LOW)]
    cot = cot_ref[...].astype(WIDE)
    for b in range(2):
        g = jnp.where(first, cols[:, 2 * b:2 * b + 1], cols[:, 2 * b + 1:2 * b + 2]) * cot
        terms = g * out_ref[b].astype(WIDE)
        heads_g = [jnp.where(first, 0.0, pltpu.roll(g, DH, 1)).astype(LOW), jnp.where(first, 0.0, g).astype(LOW)]
        deltas = [
            jnp.sum(jnp.where(first, terms, 0.0), -1, keepdims=True),
            jnp.sum(jnp.where(first, 0.0, terms), -1, keepdims=True),
        ]
        for h in range(2):
            ld = jnp.concatenate([cols[:, 4 + 2 * b + h:5 + 2 * b + h], deltas[h]], 1)
            if b == 0:
                msum_ref[h * ROWS:(h + 1) * ROWS, :] = heads_q[h]
                msum_ref[(2 + h) * ROWS:(3 + h) * ROWS, :] = heads_g[h]
                ldsum_ref[h * ROWS:(h + 1) * ROWS, :] = ld
            else:
                for s in range(SUB):
                    here = slice(s * SUB_ROWS, (s + 1) * SUB_ROWS)
                    msel_ref[s, h * SUB_ROWS:(h + 1) * SUB_ROWS, :] = heads_q[h][here]
                    msel_ref[s, (2 + h) * SUB_ROWS:(3 + h) * SUB_ROWS, :] = heads_g[h][here]
                    ldsel_ref[s, h * SUB_ROWS:(h + 1) * SUB_ROWS, :] = ld[here]


def main_kernel(place_ref, list_ref, msum_ref, msel_ref, ldsum_ref, ldsel_ref, arr_ref, hid_ref,
                dq_ref, ret_ref, kv_ref, hid_here, sem):
    load = pltpu.make_async_copy(hid_ref, hid_here, sem)
    load.start()
    base = place_ref[0] * ROWS
    scale = DH ** (-0.5)

    def grads(m, kv, seen, ld):
        half = m.shape[0] // 2
        sd = dot(m, kv, 1, 1)
        probs = jnp.where(seen, jnp.exp(sd[:half] - ld[:, :1]), 0.0)
        ds = (probs * (sd[half:] - ld[:, 1:2])).astype(LOW)
        weights = jnp.concatenate([ds, probs.astype(LOW)], 0)
        return dot(ds, kv, 1, 0), dot(weights, m, 0, 0)

    m = msum_ref[...]
    ld = ldsum_ref[...]
    row_at = lax.broadcasted_iota(jnp.int32, (2 * ROWS, 1), 0) & (ROWS - 1)
    per_one = SLOW * PER
    step = 256 // per_one
    lane = lax.broadcasted_iota(jnp.int32, (1, step * per_one), 1)
    dq_sum = jnp.zeros((2 * ROWS, PAIR), WIDE)
    for y in range(0, GROUP, step):
        kv = jnp.concatenate([arr_ref[y + k, SUMS:, :] for k in range(step)], 0)
        owner = (lane & (per_one - 1)) // PER * GROUP + y + lane // per_one
        ends = (owner * PER + (lane & (PER - 1)) + 1) * CMP - 1 - base
        dq_part, kv_grad = grads(m, kv, ends <= row_at, ld)
        dq_sum += dq_part
        low = kv_grad.astype(LOW)
        for k in range(step):
            ret_ref[y + k, SUMS:PARTS, :] = low[k * per_one:(k + 1) * per_one]
    sub_at = lax.broadcasted_iota(jnp.int32, (2 * SUB_ROWS, 1), 0) & (SUB_ROWS - 1)
    sel_lane = lax.broadcasted_iota(jnp.int32, (1, TOPN * BLK), 1)
    for s in range(SUB):
        at_key = jnp.full((1, TOPN * BLK), FAR, jnp.int32)
        places = []
        for i in range(TOPN):
            n = list_ref[s * TOPN + i]
            live = n >= 0
            owner = jnp.maximum(n, 0) // PER
            fast = owner & (GROUP - 1)
            at = pl.multiple_of(owner // GROUP * BLK, BLK)
            places.append((live, fast, at))
            kv_ref[i * BLK:(i + 1) * BLK, :] = arr_ref[fast, pl.ds(at, BLK), :]
            start = jnp.where(live, n * BLK - base - i * BLK, FAR)
            at_key = jnp.where(sel_lane // BLK == i, start, at_key)
        kv = kv_ref[...]
        seen = at_key + sel_lane <= sub_at + s * SUB_ROWS
        dq_part, kv_grad = grads(msel_ref[s], kv, seen, ldsel_ref[s])
        low = kv_grad.astype(LOW)
        for i in range(TOPN):
            live, fast, at = places[i]

            @pl.when(live)
            def _(fast=fast, at=at, i=i):
                ret_ref[fast, pl.ds(at, BLK), :] = low[i * BLK:(i + 1) * BLK]

        top = s * SUB_ROWS
        for h in range(2):
            total = dq_sum[h * ROWS + top:h * ROWS + top + SUB_ROWS, :DH]
            total = total + dq_part[h * SUB_ROWS:(h + 1) * SUB_ROWS, :DH]
            dq_ref[top:top + SUB_ROWS, h * DH:(h + 1) * DH] = total * scale
    load.wait()
    qb = dq_ref[...].astype(LOW)
    span = GROUP * COLS
    for z in range(SLOW):
        part = dot(hid_here[:, z * span:(z + 1) * span], qb, 0, 0).astype(LOW)
        for y in range(GROUP):
            ret_ref[y, PARTS + z * COLS:PARTS + (z + 1) * COLS, :] = part[y * COLS:(y + 1) * COLS]


def merge_kernel(place_ref, table_ref, in_ref, out_ref, tail_ref):
    column = place_ref[0] // GROUP * GROUP
    tail_ref[SLOW * PER:, :] = jnp.zeros((8, PAIR), WIDE)

    def add_tail(g, tail):
        return tail + in_ref[g, SUMS:PARTS, :].astype(WIDE)

    tail_ref[:SLOW * PER, :] = lax.fori_loop(
        0, GROUP, add_tail, jnp.zeros((SLOW * PER, PAIR), WIDE), unroll=8
    )
    for z in range(SLOW):

        def one(g, carry, z=z):
            sums, cols = carry
            pick = table_ref[z, column + g]
            here = in_ref[g, z * BLK:(z + 1) * BLK, :].astype(WIDE)
            sums = tuple(sums[b] + jnp.where(pick == b, here, 0.0) for b in range(PER))
            part = in_ref[g, PARTS + z * COLS:PARTS + (z + 1) * COLS, :]
            return sums, cols + part.astype(WIDE)

        zero = jnp.zeros((BLK, PAIR), WIDE)
        start = ((zero,) * PER, jnp.zeros((COLS, PAIR), WIDE))
        sums, cols = lax.fori_loop(0, GROUP, one, start, unroll=8)
        for b in range(PER):
            out_ref[z, b * BLK:(b + 1) * BLK, :] = sums[b].astype(LOW)
        out_ref[z, ROWS:ROWS + 8, :] = tail_ref[z * PER:z * PER + 8, :].astype(LOW)
        out_ref[z, ROWS + 8:, :] = cols.astype(LOW)


def final_kernel(in_ref, gk_ref, gv_ref, gw_ref):
    total = in_ref[0].astype(WIDE)
    for z in range(1, SLOW):
        total = total + in_ref[z].astype(WIDE)
    rows = [
        total[b * BLK:(b + 1) * BLK] + total[ROWS + b:ROWS + b + 1] * (1.0 / CMP) for b in range(PER)
    ]
    turned = jnp.concatenate(rows, 0).T
    gk_ref[...] = turned[:DH]
    gv_ref[...] = turned[DH:]
    gw_ref[...] = total[ROWS + 8:]


def vmem():
    return pl.BlockSpec(memory_space=pltpu.VMEM)


def smem():
    return pl.BlockSpec(memory_space=pltpu.SMEM)


def shape(*sizes, kind=LOW):
    return jax.ShapeDtypeStruct(sizes, kind)


def call(kernel, ins, outs, scratch=()):
    many = isinstance(outs, tuple)
    return pl.pallas_call(
        kernel,
        out_shape=outs,
        in_specs=ins,
        out_specs=tuple(vmem() for _ in outs) if many else vmem(),
        scratch_shapes=list(scratch),
        name=kernel.__name__,
    )


def shards(queries, keys, values, hidden, log_sums, gates, branch_out, cotangent, chosen):
    place = lax.axis_index(KV)
    here = place[None]
    lists = chosen[:, 0]
    listing = lax.dynamic_index_in_dim(lists, place, 0, keepdims=False)

    pairs, table = call(
        pairs_kernel,
        [smem(), vmem(), vmem(), vmem()],
        (shape(ROWS, PAIR), shape(SLOW, lists.shape[0], kind=jnp.int32)),
    )(here, keys.T, values.T, lists.T)
    along = lax.all_gather(pairs, KV[0], axis=0, tiled=True)
    outbound = call(relay_kernel, [smem(), smem(), vmem()], shape(GROUP, FETCH, PAIR))(here, table, along)
    arrived = lax.all_to_all(outbound, GROUP_AXES, split_axis=0, concat_axis=0, tiled=True)

    m_sum, m_sel, ld_sum, ld_sel = call(
        prep_kernel,
        [vmem()] * 5,
        (
            shape(4 * ROWS, PAIR),
            shape(SUB, 4 * SUB_ROWS, PAIR),
            shape(2 * ROWS, 2, kind=WIDE),
            shape(SUB, 2 * SUB_ROWS, 2, kind=WIDE),
        ),
    )(queries, cotangent, jnp.transpose(gates, (0, 2, 1)), jnp.transpose(log_sums, (0, 2, 1)), branch_out)
    grad_queries, returned = call(
        main_kernel,
        [smem(), smem()] + [vmem()] * 5 + [pl.BlockSpec(memory_space=pl.ANY)],
        (shape(ROWS, PAIR, kind=WIDE), shape(GROUP, BACK, PAIR)),
        (
            pltpu.VMEM((TOPN * BLK, PAIR), LOW),
            pltpu.VMEM(hidden.shape, LOW),
            pltpu.SemaphoreType.DMA,
        ),
    )(here, listing, m_sum, m_sel, ld_sum, ld_sel, arrived, hidden)
    across = lax.all_to_all(returned, GROUP_AXES, split_axis=0, concat_axis=0, tiled=True)
    merged = call(
        merge_kernel,
        [smem(), smem(), vmem()],
        shape(SLOW, LAST, PAIR),
        (pltpu.VMEM((SLOW * PER + 8, PAIR), WIDE),),
    )(here, table, across)
    home = lax.all_to_all(merged, KV[0], split_axis=0, concat_axis=0, tiled=True)
    turned_keys, turned_values, grad_weight = call(
        final_kernel,
        [vmem()],
        (shape(DH, ROWS, kind=WIDE), shape(DH, ROWS, kind=WIDE), shape(COLS, PAIR, kind=WIDE)),
    )(home)
    return (grad_queries, turned_keys.T, turned_values.T, grad_weight)


def solution(mesh):
    finer = Mesh(mesh.devices.reshape(SLOW, NEAR, 8, mesh.shape["tp"]), (*KV, "tp"))
    placed = (
        P(KV, "tp"),
        P(KV, "tp"),
        P(KV, "tp"),
        P(KV, None),
        P(None, KV, "tp"),
        P(None, KV, "tp"),
        P(None, KV, "tp"),
        P(KV, "tp"),
        P(None, "tp", None),
    )
    return jax.shard_map(
        shards,
        mesh=finer,
        in_specs=placed,
        out_specs=(P(KV, "tp"), P(KV, "tp"), P(KV, "tp"), P(KV, "tp")),
        check_vma=False,
    )
```

```python
import jax
import jax.numpy as jnp
from jax import lax
from jax.experimental import pallas as pl
from jax.experimental.pallas import tpu as pltpu
from jax.sharding import Mesh
from jax.sharding import PartitionSpec as P

DH = 64
BLK = 32
TOPN = 12
SUB = 4
CMP = 32
KV = ("kv_0", "kv_1", "kv_2")
GROUP_AXES = KV[1:]
FAR = 1 << 30
WIDE = jnp.float32
LOW = jnp.bfloat16
NEAR = 4
SLOW = 16 // NEAR
GROUP = 8 * NEAR
PER = 4
PAIR = 2 * DH
ROWS = PER * BLK
SUB_ROWS = ROWS // SUB
COLS = 16
FETCH = SLOW * (BLK + PER)
SUMS = SLOW * BLK
PARTS = SLOW * (BLK + PER)
BACK = PARTS + SLOW * COLS
LAST = ROWS + 8 + COLS


def dot(a, b, ca, cb):
    return lax.dot_general(a, b, (((ca,), (cb,)), ((), ())), preferred_element_type=WIDE)


def pairs_kernel(place_ref, keys_ref, values_ref, chosen_ref, out_ref, table_ref):
    both = jnp.concatenate([keys_ref[...], values_ref[...]], 0).astype(WIDE)
    out_ref[...] = both.T.astype(LOW)
    entry = chosen_ref[...]
    own = place_ref[0] & (GROUP - 1)
    owner = jnp.where(entry >= 0, entry // PER, -1)
    inner = entry & (PER - 1)
    for z in range(SLOW):
        hit = jnp.where(owner == z * GROUP + own, inner, PER)
        table_ref[z:z + 1, :] = jnp.min(hit, 0, keepdims=True)


def relay_kernel(place_ref, table_ref, *refs):
    *sources, out_ref = refs
    column = place_ref[0] // GROUP * GROUP
    slow_at = place_ref[0] // GROUP
    places = [(slow_at - k) & (SLOW - 1) for k in range(SLOW)]
    means = []
    for k in range(SLOW):
        rows = sources[k][...].astype(WIDE).reshape(PER, CMP, PAIR)
        means.append(jnp.mean(rows, 1))
    ordered = []
    for z in range(SLOW):
        pick = jnp.zeros((PER, PAIR), WIDE)
        for k in range(SLOW):
            pick = jnp.where(places[k] == z, means[k], pick)
        ordered.append(pick)
    low = jnp.concatenate(ordered, 0).astype(LOW)

    def one(g, carry):
        out_ref[g, SUMS:, :] = low
        for k in range(SLOW):
            z = places[k]
            pick = jnp.minimum(table_ref[z, column + g], PER - 1)
            at = pl.multiple_of(pick * BLK, BLK)
            out_ref[g, pl.ds(pl.multiple_of(z * BLK, BLK), BLK), :] = sources[k][pl.ds(at, BLK), :]
        return carry

    lax.fori_loop(0, GROUP, one, 0, unroll=2)


def prep_kernel(q_ref, cot_ref, gates_ref, logs_ref, out_ref, msum_ref, msel_ref, ldsum_ref, ldsel_ref):
    cols = jnp.concatenate([gates_ref[0], gates_ref[1], logs_ref[0], logs_ref[1]], 0).T
    first = lax.broadcasted_iota(jnp.int32, (ROWS, PAIR), 1) < DH
    q = q_ref[...].astype(WIDE) * (DH ** (-0.5))
    heads_q = [jnp.where(first, q, 0.0).astype(LOW), jnp.where(first, pltpu.roll(q, DH, 1), 0.0).astype(LOW)]
    cot = cot_ref[...].astype(WIDE)
    for b in range(2):
        g = jnp.where(first, cols[:, 2 * b:2 * b + 1], cols[:, 2 * b + 1:2 * b + 2]) * cot
        terms = g * out_ref[b].astype(WIDE)
        heads_g = [jnp.where(first, 0.0, pltpu.roll(g, DH, 1)).astype(LOW), jnp.where(first, 0.0, g).astype(LOW)]
        deltas = [
            jnp.sum(jnp.where(first, terms, 0.0), -1, keepdims=True),
            jnp.sum(jnp.where(first, 0.0, terms), -1, keepdims=True),
        ]
        for h in range(2):
            ld = jnp.concatenate([cols[:, 4 + 2 * b + h:5 + 2 * b + h], deltas[h]], 1)
            if b == 0:
                msum_ref[h * ROWS:(h + 1) * ROWS, :] = heads_q[h]
                msum_ref[(2 + h) * ROWS:(3 + h) * ROWS, :] = heads_g[h]
                ldsum_ref[h * ROWS:(h + 1) * ROWS, :] = ld
            else:
                for s in range(SUB):
                    here = slice(s * SUB_ROWS, (s + 1) * SUB_ROWS)
                    msel_ref[s, h * SUB_ROWS:(h + 1) * SUB_ROWS, :] = heads_q[h][here]
                    msel_ref[s, (2 + h) * SUB_ROWS:(3 + h) * SUB_ROWS, :] = heads_g[h][here]
                    ldsel_ref[s, h * SUB_ROWS:(h + 1) * SUB_ROWS, :] = ld[here]


def main_kernel(place_ref, list_ref, msum_ref, msel_ref, ldsum_ref, ldsel_ref, arr_ref, hid_ref,
                dq_ref, ret_ref, kv_ref, hid_here, sem):
    load = pltpu.make_async_copy(hid_ref, hid_here, sem)
    load.start()
    base = place_ref[0] * ROWS
    scale = DH ** (-0.5)

    def grads(m, kv, seen, ld):
        half = m.shape[0] // 2
        sd = dot(m, kv, 1, 1)
        probs = jnp.where(seen, jnp.exp(sd[:half] - ld[:, :1]), 0.0)
        ds = (probs * (sd[half:] - ld[:, 1:2])).astype(LOW)
        weights = jnp.concatenate([ds, probs.astype(LOW)], 0)
        return dot(ds, kv, 1, 0), dot(weights, m, 0, 0)

    m = msum_ref[...]
    ld = ldsum_ref[...]
    row_at = lax.broadcasted_iota(jnp.int32, (2 * ROWS, 1), 0) & (ROWS - 1)
    per_one = SLOW * PER
    step = 256 // per_one
    lane = lax.broadcasted_iota(jnp.int32, (1, step * per_one), 1)
    dq_sum = jnp.zeros((2 * ROWS, PAIR), WIDE)
    for y in range(0, GROUP, step):
        kv = jnp.concatenate([arr_ref[y + k, SUMS:, :] for k in range(step)], 0)
        owner = (lane & (per_one - 1)) // PER * GROUP + y + lane // per_one
        ends = (owner * PER + (lane & (PER - 1)) + 1) * CMP - 1 - base
        dq_part, kv_grad = grads(m, kv, ends <= row_at, ld)
        dq_sum += dq_part
        low = kv_grad.astype(LOW)
        for k in range(step):
            ret_ref[y + k, SUMS:PARTS, :] = low[k * per_one:(k + 1) * per_one]
    sub_at = lax.broadcasted_iota(jnp.int32, (2 * SUB_ROWS, 1), 0) & (SUB_ROWS - 1)
    sel_lane = lax.broadcasted_iota(jnp.int32, (1, TOPN * BLK), 1)
    for s in range(SUB):
        at_key = jnp.full((1, TOPN * BLK), FAR, jnp.int32)
        places = []
        for i in range(TOPN):
            n = list_ref[s * TOPN + i]
            live = n >= 0
            owner = jnp.maximum(n, 0) // PER
            fast = owner & (GROUP - 1)
            at = pl.multiple_of(owner // GROUP * BLK, BLK)
            places.append((live, fast, at))
            kv_ref[i * BLK:(i + 1) * BLK, :] = arr_ref[fast, pl.ds(at, BLK), :]
            start = jnp.where(live, n * BLK - base - i * BLK, FAR)
            at_key = jnp.where(sel_lane // BLK == i, start, at_key)
        kv = kv_ref[...]
        seen = at_key + sel_lane <= sub_at + s * SUB_ROWS
        dq_part, kv_grad = grads(msel_ref[s], kv, seen, ldsel_ref[s])
        low = kv_grad.astype(LOW)
        for i in range(TOPN):
            live, fast, at = places[i]

            @pl.when(live)
            def _(fast=fast, at=at, i=i):
                ret_ref[fast, pl.ds(at, BLK), :] = low[i * BLK:(i + 1) * BLK]

        top = s * SUB_ROWS
        for h in range(2):
            total = dq_sum[h * ROWS + top:h * ROWS + top + SUB_ROWS, :DH]
            total = total + dq_part[h * SUB_ROWS:(h + 1) * SUB_ROWS, :DH]
            dq_ref[top:top + SUB_ROWS, h * DH:(h + 1) * DH] = total * scale
    load.wait()
    qb = dq_ref[...].astype(LOW)
    span = GROUP * COLS
    for z in range(SLOW):
        part = dot(hid_here[:, z * span:(z + 1) * span], qb, 0, 0).astype(LOW)
        for y in range(GROUP):
            ret_ref[y, PARTS + z * COLS:PARTS + (z + 1) * COLS, :] = part[y * COLS:(y + 1) * COLS]


def merge_kernel(place_ref, table_ref, in_ref, *refs):
    *outs, tail_ref = refs
    column = place_ref[0] // GROUP * GROUP
    slow_at = place_ref[0] // GROUP
    tail_ref[SLOW * PER:, :] = jnp.zeros((8, PAIR), WIDE)

    def add_tail(g, tail):
        return tail + in_ref[g, SUMS:PARTS, :].astype(WIDE)

    tail_ref[:SLOW * PER, :] = lax.fori_loop(
        0, GROUP, add_tail, jnp.zeros((SLOW * PER, PAIR), WIDE), unroll=8
    )
    for k in range(SLOW):
        z = (slow_at + k) & (SLOW - 1)
        block_at = pl.multiple_of(z * BLK, BLK)
        part_at = pl.multiple_of(PARTS + z * COLS, COLS)

        def one(g, carry):
            sums, cols = carry
            pick = table_ref[z, column + g]
            here = in_ref[g, pl.ds(block_at, BLK), :].astype(WIDE)
            sums = tuple(sums[b] + jnp.where(pick == b, here, 0.0) for b in range(PER))
            return sums, cols + in_ref[g, pl.ds(part_at, COLS), :].astype(WIDE)

        zero = jnp.zeros((BLK, PAIR), WIDE)
        start = ((zero,) * PER, jnp.zeros((COLS, PAIR), WIDE))
        sums, cols = lax.fori_loop(0, GROUP, one, start, unroll=8)
        for b in range(PER):
            outs[k][b * BLK:(b + 1) * BLK, :] = sums[b].astype(LOW)
        outs[k][ROWS:ROWS + 8, :] = tail_ref[pl.ds(z * PER, 8), :].astype(LOW)
        outs[k][ROWS + 8:, :] = cols.astype(LOW)


def final_kernel(*refs):
    *ins, gk_ref, gv_ref, gw_ref = refs
    total = ins[0][...].astype(WIDE)
    for ref in ins[1:]:
        total = total + ref[...].astype(WIDE)
    rows = [
        total[b * BLK:(b + 1) * BLK] + total[ROWS + b:ROWS + b + 1] * (1.0 / CMP) for b in range(PER)
    ]
    turned = jnp.concatenate(rows, 0).T
    gk_ref[...] = turned[:DH]
    gv_ref[...] = turned[DH:]
    gw_ref[...] = total[ROWS + 8:]


def moved(array, by):
    return lax.ppermute(array, KV[0], [(i, (i + by) % SLOW) for i in range(SLOW)])


def vmem():
    return pl.BlockSpec(memory_space=pltpu.VMEM)


def smem():
    return pl.BlockSpec(memory_space=pltpu.SMEM)


def shape(*sizes, kind=LOW):
    return jax.ShapeDtypeStruct(sizes, kind)


def call(kernel, ins, outs, scratch=()):
    many = isinstance(outs, tuple)
    return pl.pallas_call(
        kernel,
        out_shape=outs,
        in_specs=ins,
        out_specs=tuple(vmem() for _ in outs) if many else vmem(),
        scratch_shapes=list(scratch),
        name=kernel.__name__,
    )


def shards(queries, keys, values, hidden, log_sums, gates, branch_out, cotangent, chosen):
    place = lax.axis_index(KV)
    here = place[None]
    lists = chosen[:, 0]
    listing = lax.dynamic_index_in_dim(lists, place, 0, keepdims=False)

    pairs, table = call(
        pairs_kernel,
        [smem(), vmem(), vmem(), vmem()],
        (shape(ROWS, PAIR), shape(SLOW, lists.shape[0], kind=jnp.int32)),
    )(here, keys.T, values.T, lists.T)
    along = [pairs] + [moved(pairs, by) for by in range(1, SLOW)]
    outbound = call(relay_kernel, [smem(), smem()] + [vmem()] * SLOW, shape(GROUP, FETCH, PAIR))(
        here, table, *along
    )
    arrived = lax.all_to_all(outbound, GROUP_AXES, split_axis=0, concat_axis=0, tiled=True)

    m_sum, m_sel, ld_sum, ld_sel = call(
        prep_kernel,
        [vmem()] * 5,
        (
            shape(4 * ROWS, PAIR),
            shape(SUB, 4 * SUB_ROWS, PAIR),
            shape(2 * ROWS, 2, kind=WIDE),
            shape(SUB, 2 * SUB_ROWS, 2, kind=WIDE),
        ),
    )(queries, cotangent, jnp.transpose(gates, (0, 2, 1)), jnp.transpose(log_sums, (0, 2, 1)), branch_out)
    grad_queries, returned = call(
        main_kernel,
        [smem(), smem()] + [vmem()] * 5 + [pl.BlockSpec(memory_space=pl.ANY)],
        (shape(ROWS, PAIR, kind=WIDE), shape(GROUP, BACK, PAIR)),
        (
            pltpu.VMEM((TOPN * BLK, PAIR), LOW),
            pltpu.VMEM(hidden.shape, LOW),
            pltpu.SemaphoreType.DMA,
        ),
    )(here, listing, m_sum, m_sel, ld_sum, ld_sel, arrived, hidden)
    across = lax.all_to_all(returned, GROUP_AXES, split_axis=0, concat_axis=0, tiled=True)
    merged = call(
        merge_kernel,
        [smem(), smem(), vmem()],
        (shape(LAST, PAIR),) * SLOW,
        (pltpu.VMEM((SLOW * PER + 8, PAIR), WIDE),),
    )(here, table, across)
    home = [merged[0]] + [moved(merged[by], by) for by in range(1, SLOW)]
    turned_keys, turned_values, grad_weight = call(
        final_kernel,
        [vmem()] * SLOW,
        (shape(DH, ROWS, kind=WIDE), shape(DH, ROWS, kind=WIDE), shape(COLS, PAIR, kind=WIDE)),
    )(*home)
    return (grad_queries, turned_keys.T, turned_values.T, grad_weight)


def solution(mesh):
    finer = Mesh(mesh.devices.reshape(SLOW, NEAR, 8, mesh.shape["tp"]), (*KV, "tp"))
    placed = (
        P(KV, "tp"),
        P(KV, "tp"),
        P(KV, "tp"),
        P(KV, None),
        P(None, KV, "tp"),
        P(None, KV, "tp"),
        P(None, KV, "tp"),
        P(KV, "tp"),
        P(None, "tp", None),
    )
    return jax.shard_map(
        shards,
        mesh=finer,
        in_specs=placed,
        out_specs=(P(KV, "tp"), P(KV, "tp"), P(KV, "tp"), P(KV, "tp")),
        check_vma=False,
    )
```

```python
import jax
import jax.numpy as jnp
from jax import lax
from jax.experimental import pallas as pl
from jax.experimental.pallas import tpu as pltpu
from jax.sharding import Mesh
from jax.sharding import PartitionSpec as P

DH = 64
BLK = 32
TOPN = 12
SUB = 4
CMP = 32
KV = ("kv_0", "kv_1", "kv_2")
GROUP_AXES = KV[1:]
FAR = 1 << 30
WIDE = jnp.float32
LOW = jnp.bfloat16
NEAR = 4
SLOW = 16 // NEAR
GROUP = 8 * NEAR
PER = 4
PAIR = 2 * DH
ROWS = PER * BLK
SUB_ROWS = ROWS // SUB
COLS = 16
FETCH = SLOW * (BLK + PER)
SUMS = SLOW * BLK
PARTS = SLOW * (BLK + PER)
BACK = PARTS + SLOW * COLS
LAST = ROWS + 8 + COLS


def dot(a, b, ca, cb):
    return lax.dot_general(a, b, (((ca,), (cb,)), ((), ())), preferred_element_type=WIDE)


def pairs_kernel(place_ref, keys_ref, values_ref, chosen_ref, out_ref, table_ref):
    both = jnp.concatenate([keys_ref[...], values_ref[...]], 0).astype(WIDE)
    out_ref[...] = both.T.astype(LOW)
    entry = chosen_ref[...]
    own = place_ref[0] & (GROUP - 1)
    owner = jnp.where(entry >= 0, entry // PER, -1)
    inner = entry & (PER - 1)
    for z in range(SLOW):
        hit = jnp.where(owner == z * GROUP + own, inner, PER)
        table_ref[z:z + 1, :] = jnp.min(hit, 0, keepdims=True)


def relay_kernel(place_ref, table_ref, all_ref, out_ref):
    column = place_ref[0] // GROUP * GROUP
    rows = all_ref[...].astype(WIDE).reshape(SLOW * PER, CMP, PAIR)
    means = jnp.mean(rows, 1).astype(LOW)

    def one(g, carry):
        out_ref[g, SUMS:, :] = means
        for z in range(SLOW):
            pick = jnp.minimum(table_ref[z, column + g], PER - 1)
            at = pl.multiple_of((z * PER + pick) * BLK, BLK)
            out_ref[g, z * BLK:(z + 1) * BLK, :] = all_ref[pl.ds(at, BLK), :]
        return carry

    lax.fori_loop(0, GROUP, one, 0, unroll=2)


def prep_kernel(q_ref, cot_ref, gates_ref, logs_ref, out_ref, msum_ref, msel_ref, ldsum_ref, ldsel_ref):
    cols = jnp.concatenate([gates_ref[0], gates_ref[1], logs_ref[0], logs_ref[1]], 0).T
    first = lax.broadcasted_iota(jnp.int32, (ROWS, PAIR), 1) < DH
    q = q_ref[...].astype(WIDE) * (DH ** (-0.5))
    heads_q = [jnp.where(first, q, 0.0).astype(LOW), jnp.where(first, pltpu.roll(q, DH, 1), 0.0).astype(LOW)]
    cot = cot_ref[...].astype(WIDE)
    for b in range(2):
        g = jnp.where(first, cols[:, 2 * b:2 * b + 1], cols[:, 2 * b + 1:2 * b + 2]) * cot
        terms = g * out_ref[b].astype(WIDE)
        heads_g = [jnp.where(first, 0.0, pltpu.roll(g, DH, 1)).astype(LOW), jnp.where(first, 0.0, g).astype(LOW)]
        deltas = [
            jnp.sum(jnp.where(first, terms, 0.0), -1, keepdims=True),
            jnp.sum(jnp.where(first, 0.0, terms), -1, keepdims=True),
        ]
        for h in range(2):
            ld = jnp.concatenate([cols[:, 4 + 2 * b + h:5 + 2 * b + h], deltas[h]], 1)
            if b == 0:
                msum_ref[h * ROWS:(h + 1) * ROWS, :] = heads_q[h]
                msum_ref[(2 + h) * ROWS:(3 + h) * ROWS, :] = heads_g[h]
                ldsum_ref[h * ROWS:(h + 1) * ROWS, :] = ld
            else:
                for s in range(SUB):
                    here = slice(s * SUB_ROWS, (s + 1) * SUB_ROWS)
                    msel_ref[s, h * SUB_ROWS:(h + 1) * SUB_ROWS, :] = heads_q[h][here]
                    msel_ref[s, (2 + h) * SUB_ROWS:(3 + h) * SUB_ROWS, :] = heads_g[h][here]
                    ldsel_ref[s, h * SUB_ROWS:(h + 1) * SUB_ROWS, :] = ld[here]


def main_kernel(place_ref, list_ref, msum_ref, msel_ref, ldsum_ref, ldsel_ref, arr_ref, hid_ref,
                dq_ref, ret_ref, kv_ref):
    base = place_ref[0] * ROWS
    scale = DH ** (-0.5)

    def grads(m, kv, seen, ld):
        half = m.shape[0] // 2
        sd = dot(m, kv, 1, 1)
        probs = jnp.where(seen, jnp.exp(sd[:half] - ld[:, :1]), 0.0)
        ds = (probs * (sd[half:] - ld[:, 1:2])).astype(LOW)
        weights = jnp.concatenate([ds, probs.astype(LOW)], 0)
        return dot(ds, kv, 1, 0), dot(weights, m, 0, 0)

    m = msum_ref[...]
    ld = ldsum_ref[...]
    row_at = lax.broadcasted_iota(jnp.int32, (2 * ROWS, 1), 0) & (ROWS - 1)
    per_one = SLOW * PER
    step = 256 // per_one
    lane = lax.broadcasted_iota(jnp.int32, (1, step * per_one), 1)
    dq_sum = jnp.zeros((2 * ROWS, PAIR), WIDE)
    for y in range(0, GROUP, step):
        kv = jnp.concatenate([arr_ref[y + k, SUMS:, :] for k in range(step)], 0)
        owner = (lane & (per_one - 1)) // PER * GROUP + y + lane // per_one
        ends = (owner * PER + (lane & (PER - 1)) + 1) * CMP - 1 - base
        dq_part, kv_grad = grads(m, kv, ends <= row_at, ld)
        dq_sum += dq_part
        low = kv_grad.astype(LOW)
        for k in range(step):
            ret_ref[y + k, SUMS:PARTS, :] = low[k * per_one:(k + 1) * per_one]
    sub_at = lax.broadcasted_iota(jnp.int32, (2 * SUB_ROWS, 1), 0) & (SUB_ROWS - 1)
    sel_lane = lax.broadcasted_iota(jnp.int32, (1, TOPN * BLK), 1)
    for s in range(SUB):
        at_key = jnp.full((1, TOPN * BLK), FAR, jnp.int32)
        places = []
        for i in range(TOPN):
            n = list_ref[s * TOPN + i]
            live = n >= 0
            owner = jnp.maximum(n, 0) // PER
            fast = owner & (GROUP - 1)
            at = pl.multiple_of(owner // GROUP * BLK, BLK)
            places.append((live, fast, at))
            kv_ref[i * BLK:(i + 1) * BLK, :] = arr_ref[fast, pl.ds(at, BLK), :]
            start = jnp.where(live, n * BLK - base - i * BLK, FAR)
            at_key = jnp.where(sel_lane // BLK == i, start, at_key)
        kv = kv_ref[...]
        seen = at_key + sel_lane <= sub_at + s * SUB_ROWS
        dq_part, kv_grad = grads(msel_ref[s], kv, seen, ldsel_ref[s])
        low = kv_grad.astype(LOW)
        for i in range(TOPN):
            live, fast, at = places[i]

            @pl.when(live)
            def _(fast=fast, at=at, i=i):
                ret_ref[fast, pl.ds(at, BLK), :] = low[i * BLK:(i + 1) * BLK]

        top = s * SUB_ROWS
        for h in range(2):
            total = dq_sum[h * ROWS + top:h * ROWS + top + SUB_ROWS, :DH]
            total = total + dq_part[h * SUB_ROWS:(h + 1) * SUB_ROWS, :DH]
            dq_ref[top:top + SUB_ROWS, h * DH:(h + 1) * DH] = total * scale
    qb = dq_ref[...].astype(LOW)
    span = GROUP * COLS
    for z in range(SLOW):
        part = dot(hid_ref[:, z * span:(z + 1) * span], qb, 0, 0).astype(LOW)
        for y in range(GROUP):
            ret_ref[y, PARTS + z * COLS:PARTS + (z + 1) * COLS, :] = part[y * COLS:(y + 1) * COLS]


def merge_kernel(place_ref, table_ref, in_ref, out_ref, tail_ref):
    column = place_ref[0] // GROUP * GROUP
    tail_ref[SLOW * PER:, :] = jnp.zeros((8, PAIR), WIDE)

    def add_tail(g, tail):
        return tail + in_ref[g, SUMS:PARTS, :].astype(WIDE)

    tail_ref[:SLOW * PER, :] = lax.fori_loop(
        0, GROUP, add_tail, jnp.zeros((SLOW * PER, PAIR), WIDE), unroll=8
    )
    for z in range(SLOW):

        def one(g, carry, z=z):
            sums, cols = carry
            pick = table_ref[z, column + g]
            here = in_ref[g, z * BLK:(z + 1) * BLK, :].astype(WIDE)
            sums = tuple(sums[b] + jnp.where(pick == b, here, 0.0) for b in range(PER))
            part = in_ref[g, PARTS + z * COLS:PARTS + (z + 1) * COLS, :]
            return sums, cols + part.astype(WIDE)

        zero = jnp.zeros((BLK, PAIR), WIDE)
        start = ((zero,) * PER, jnp.zeros((COLS, PAIR), WIDE))
        sums, cols = lax.fori_loop(0, GROUP, one, start, unroll=8)
        for b in range(PER):
            out_ref[z, b * BLK:(b + 1) * BLK, :] = sums[b].astype(LOW)
        out_ref[z, ROWS:ROWS + 8, :] = tail_ref[z * PER:z * PER + 8, :].astype(LOW)
        out_ref[z, ROWS + 8:, :] = cols.astype(LOW)


def final_kernel(in_ref, gk_ref, gv_ref, gw_ref):
    total = in_ref[0].astype(WIDE)
    for z in range(1, SLOW):
        total = total + in_ref[z].astype(WIDE)
    rows = [
        total[b * BLK:(b + 1) * BLK] + total[ROWS + b:ROWS + b + 1] * (1.0 / CMP) for b in range(PER)
    ]
    turned = jnp.concatenate(rows, 0).T
    gk_ref[...] = turned[:DH]
    gv_ref[...] = turned[DH:]
    gw_ref[...] = total[ROWS + 8:]


def vmem():
    return pl.BlockSpec(memory_space=pltpu.VMEM)


def smem():
    return pl.BlockSpec(memory_space=pltpu.SMEM)


def shape(*sizes, kind=LOW):
    return jax.ShapeDtypeStruct(sizes, kind)


def local(*sizes, kind=LOW):
    return pltpu.VMEM(sizes, kind)


def inside(*arrays):
    return [pltpu.with_memory_space_constraint(array, pltpu.VMEM) for array in arrays]


def call(kernel, ins, outs, scratch=()):
    many = isinstance(outs, tuple)
    return pl.pallas_call(
        kernel,
        out_shape=outs,
        in_specs=ins,
        out_specs=tuple(vmem() for _ in outs) if many else vmem(),
        scratch_shapes=list(scratch),
        compiler_params=pltpu.CompilerParams(vmem_limit_bytes=16 << 20),
        name=kernel.__name__,
    )


def shards(queries, keys, values, hidden, log_sums, gates, branch_out, cotangent, chosen):
    place = lax.axis_index(KV)
    here = place[None]
    lists = chosen[:, 0]
    listing = lax.dynamic_index_in_dim(lists, place, 0, keepdims=False)

    pairs, table = call(
        pairs_kernel,
        [smem(), vmem(), vmem(), vmem()],
        (local(ROWS, PAIR), shape(SLOW, lists.shape[0], kind=jnp.int32)),
    )(here, keys.T, values.T, lists.T)
    along = lax.all_gather(pairs, KV[0], axis=0, tiled=True)
    outbound = call(relay_kernel, [smem(), smem(), vmem()], local(GROUP, FETCH, PAIR))(here, table, *inside(along))
    arrived = lax.all_to_all(outbound, GROUP_AXES, split_axis=0, concat_axis=0, tiled=True)

    m_sum, m_sel, ld_sum, ld_sel = call(
        prep_kernel,
        [vmem()] * 5,
        (
            local(4 * ROWS, PAIR),
            local(SUB, 4 * SUB_ROWS, PAIR),
            local(2 * ROWS, 2, kind=WIDE),
            local(SUB, 2 * SUB_ROWS, 2, kind=WIDE),
        ),
    )(queries, cotangent, jnp.transpose(gates, (0, 2, 1)), jnp.transpose(log_sums, (0, 2, 1)), branch_out)
    grad_queries, returned = call(
        main_kernel,
        [smem(), smem()] + [vmem()] * 6,
        (shape(ROWS, PAIR, kind=WIDE), local(GROUP, BACK, PAIR)),
        (pltpu.VMEM((TOPN * BLK, PAIR), LOW),),
    )(here, listing, *inside(m_sum, m_sel, ld_sum, ld_sel, arrived, hidden))
    across = lax.all_to_all(returned, GROUP_AXES, split_axis=0, concat_axis=0, tiled=True)
    merged = call(
        merge_kernel,
        [smem(), smem(), vmem()],
        local(SLOW, LAST, PAIR),
        (pltpu.VMEM((SLOW * PER + 8, PAIR), WIDE),),
    )(here, table, *inside(across))
    home = lax.all_to_all(merged, KV[0], split_axis=0, concat_axis=0, tiled=True)
    turned_keys, turned_values, grad_weight = call(
        final_kernel,
        [vmem()],
        (shape(DH, ROWS, kind=WIDE), shape(DH, ROWS, kind=WIDE), shape(COLS, PAIR, kind=WIDE)),
    )(*inside(home))
    return (grad_queries, turned_keys.T, turned_values.T, grad_weight)


def solution(mesh):
    finer = Mesh(mesh.devices.reshape(SLOW, NEAR, 8, mesh.shape["tp"]), (*KV, "tp"))
    placed = (
        P(KV, "tp"),
        P(KV, "tp"),
        P(KV, "tp"),
        P(KV, None),
        P(None, KV, "tp"),
        P(None, KV, "tp"),
        P(None, KV, "tp"),
        P(KV, "tp"),
        P(None, "tp", None),
    )
    return jax.shard_map(
        shards,
        mesh=finer,
        in_specs=placed,
        out_specs=(P(KV, "tp"), P(KV, "tp"), P(KV, "tp"), P(KV, "tp")),
        check_vma=False,
    )
```

```python
import jax
import jax.numpy as jnp
from jax import lax
from jax.experimental import pallas as pl
from jax.experimental.pallas import tpu as pltpu
from jax.sharding import Mesh
from jax.sharding import PartitionSpec as P

DH = 64
BLK = 32
TOPN = 12
SUB = 4
CMP = 32
KV = ("kv_0", "kv_1", "kv_2")
GROUP_AXES = KV[1:]
FAR = 1 << 30
WIDE = jnp.float32
LOW = jnp.bfloat16
NEAR = 2
SLOW = 16 // NEAR
GROUP = 8 * NEAR
PER = 4
PAIR = 2 * DH
ROWS = PER * BLK
SUB_ROWS = ROWS // SUB
COLS = 16
FETCH = SLOW * (BLK + PER)
SUMS = SLOW * BLK
PARTS = SLOW * (BLK + PER)
BACK = PARTS + SLOW * COLS
LAST = ROWS + 8 + COLS


def dot(a, b, ca, cb):
    return lax.dot_general(a, b, (((ca,), (cb,)), ((), ())), preferred_element_type=WIDE)


def pairs_kernel(place_ref, keys_ref, values_ref, chosen_ref, out_ref, table_ref, list_ref, turned_ref):
    both = jnp.concatenate([keys_ref[...], values_ref[...]], 0).astype(WIDE)
    out_ref[...] = both.T.astype(LOW)
    entry = chosen_ref[...]
    turned_ref[...] = entry.T
    list_ref[...] = turned_ref[pl.ds(place_ref[0], 1), :]
    own = place_ref[0] & (GROUP - 1)
    owner = jnp.where(entry >= 0, entry // PER, -1)
    inner = entry & (PER - 1)
    for z in range(SLOW):
        hit = jnp.where(owner == z * GROUP + own, inner, PER)
        table_ref[z:z + 1, :] = jnp.min(hit, 0, keepdims=True)


def relay_kernel(place_ref, table_ref, all_ref, out_ref):
    column = place_ref[0] // GROUP * GROUP
    rows = all_ref[...].astype(WIDE).reshape(SLOW * PER, CMP, PAIR)
    means = jnp.mean(rows, 1).astype(LOW)

    def one(g, carry):
        out_ref[g, SUMS:, :] = means
        for z in range(SLOW):
            pick = jnp.minimum(table_ref[z, column + g], PER - 1)
            at = pl.multiple_of((z * PER + pick) * BLK, BLK)
            out_ref[g, z * BLK:(z + 1) * BLK, :] = all_ref[pl.ds(at, BLK), :]
        return carry

    lax.fori_loop(0, GROUP, one, 0, unroll=2)


def prep_kernel(q_ref, cot_ref, gates_ref, logs_ref, out_ref, msum_ref, msel_ref, ldsum_ref, ldsel_ref):
    cols = jnp.concatenate([gates_ref[0], gates_ref[1], logs_ref[0], logs_ref[1]], 0).T
    first = lax.broadcasted_iota(jnp.int32, (ROWS, PAIR), 1) < DH
    q = q_ref[...].astype(WIDE) * (DH ** (-0.5))
    heads_q = [jnp.where(first, q, 0.0).astype(LOW), jnp.where(first, pltpu.roll(q, DH, 1), 0.0).astype(LOW)]
    cot = cot_ref[...].astype(WIDE)
    for b in range(2):
        g = jnp.where(first, cols[:, 2 * b:2 * b + 1], cols[:, 2 * b + 1:2 * b + 2]) * cot
        terms = g * out_ref[b].astype(WIDE)
        heads_g = [jnp.where(first, 0.0, pltpu.roll(g, DH, 1)).astype(LOW), jnp.where(first, 0.0, g).astype(LOW)]
        deltas = [
            jnp.sum(jnp.where(first, terms, 0.0), -1, keepdims=True),
            jnp.sum(jnp.where(first, 0.0, terms), -1, keepdims=True),
        ]
        for h in range(2):
            ld = jnp.concatenate([cols[:, 4 + 2 * b + h:5 + 2 * b + h], deltas[h]], 1)
            if b == 0:
                msum_ref[h * ROWS:(h + 1) * ROWS, :] = heads_q[h]
                msum_ref[(2 + h) * ROWS:(3 + h) * ROWS, :] = heads_g[h]
                ldsum_ref[h * ROWS:(h + 1) * ROWS, :] = ld
            else:
                for s in range(SUB):
                    here = slice(s * SUB_ROWS, (s + 1) * SUB_ROWS)
                    msel_ref[s, h * SUB_ROWS:(h + 1) * SUB_ROWS, :] = heads_q[h][here]
                    msel_ref[s, (2 + h) * SUB_ROWS:(3 + h) * SUB_ROWS, :] = heads_g[h][here]
                    ldsel_ref[s, h * SUB_ROWS:(h + 1) * SUB_ROWS, :] = ld[here]


def main_kernel(place_ref, list_ref, msum_ref, msel_ref, ldsum_ref, ldsel_ref, arr_ref, hid_ref,
                dq_ref, ret_ref, kv_ref):
    base = place_ref[0] * ROWS
    scale = DH ** (-0.5)

    def grads(m, kv, seen, ld):
        half = m.shape[0] // 2
        sd = dot(m, kv, 1, 1)
        probs = jnp.where(seen, jnp.exp(sd[:half] - ld[:, :1]), 0.0)
        ds = (probs * (sd[half:] - ld[:, 1:2])).astype(LOW)
        weights = jnp.concatenate([ds, probs.astype(LOW)], 0)
        return dot(ds, kv, 1, 0), dot(weights, m, 0, 0)

    m = msum_ref[...]
    ld = ldsum_ref[...]
    row_at = lax.broadcasted_iota(jnp.int32, (2 * ROWS, 1), 0) & (ROWS - 1)
    per_one = SLOW * PER
    step = 256 // per_one
    lane = lax.broadcasted_iota(jnp.int32, (1, step * per_one), 1)
    dq_sum = jnp.zeros((2 * ROWS, PAIR), WIDE)
    for y in range(0, GROUP, step):
        kv = jnp.concatenate([arr_ref[y + k, SUMS:, :] for k in range(step)], 0)
        owner = (lane & (per_one - 1)) // PER * GROUP + y + lane // per_one
        ends = (owner * PER + (lane & (PER - 1)) + 1) * CMP - 1 - base
        dq_part, kv_grad = grads(m, kv, ends <= row_at, ld)
        dq_sum += dq_part
        low = kv_grad.astype(LOW)
        for k in range(step):
            ret_ref[y + k, SUMS:PARTS, :] = low[k * per_one:(k + 1) * per_one]
    sub_at = lax.broadcasted_iota(jnp.int32, (2 * SUB_ROWS, 1), 0) & (SUB_ROWS - 1)
    sel_lane = lax.broadcasted_iota(jnp.int32, (1, TOPN * BLK), 1)
    for s in range(SUB):
        at_key = jnp.full((1, TOPN * BLK), FAR, jnp.int32)
        places = []
        for i in range(TOPN):
            n = list_ref[0, s * TOPN + i]
            live = n >= 0
            owner = jnp.maximum(n, 0) // PER
            fast = owner & (GROUP - 1)
            at = pl.multiple_of(owner // GROUP * BLK, BLK)
            places.append((live, fast, at))
            kv_ref[i * BLK:(i + 1) * BLK, :] = arr_ref[fast, pl.ds(at, BLK), :]
            start = jnp.where(live, n * BLK - base - i * BLK, FAR)
            at_key = jnp.where(sel_lane // BLK == i, start, at_key)
        kv = kv_ref[...]
        seen = at_key + sel_lane <= sub_at + s * SUB_ROWS
        dq_part, kv_grad = grads(msel_ref[s], kv, seen, ldsel_ref[s])
        low = kv_grad.astype(LOW)
        for i in range(TOPN):
            live, fast, at = places[i]

            @pl.when(live)
            def _(fast=fast, at=at, i=i):
                ret_ref[fast, pl.ds(at, BLK), :] = low[i * BLK:(i + 1) * BLK]

        top = s * SUB_ROWS
        for h in range(2):
            total = dq_sum[h * ROWS + top:h * ROWS + top + SUB_ROWS, :DH]
            total = total + dq_part[h * SUB_ROWS:(h + 1) * SUB_ROWS, :DH]
            dq_ref[top:top + SUB_ROWS, h * DH:(h + 1) * DH] = total * scale
    qb = dq_ref[...].astype(LOW)
    span = GROUP * COLS
    for z in range(SLOW):
        part = dot(hid_ref[:, z * span:(z + 1) * span], qb, 0, 0).astype(LOW)
        for y in range(GROUP):
            ret_ref[y, PARTS + z * COLS:PARTS + (z + 1) * COLS, :] = part[y * COLS:(y + 1) * COLS]


def merge_kernel(place_ref, table_ref, in_ref, out_ref, tail_ref):
    column = place_ref[0] // GROUP * GROUP
    tail_ref[SLOW * PER:, :] = jnp.zeros((8, PAIR), WIDE)

    def add_tail(g, tail):
        return tail + in_ref[g, SUMS:PARTS, :].astype(WIDE)

    tail_ref[:SLOW * PER, :] = lax.fori_loop(
        0, GROUP, add_tail, jnp.zeros((SLOW * PER, PAIR), WIDE), unroll=8
    )
    for z in range(SLOW):

        def one(g, carry, z=z):
            sums, cols = carry
            pick = table_ref[z, column + g]
            here = in_ref[g, z * BLK:(z + 1) * BLK, :].astype(WIDE)
            sums = tuple(sums[b] + jnp.where(pick == b, here, 0.0) for b in range(PER))
            part = in_ref[g, PARTS + z * COLS:PARTS + (z + 1) * COLS, :]
            return sums, cols + part.astype(WIDE)

        zero = jnp.zeros((BLK, PAIR), WIDE)
        start = ((zero,) * PER, jnp.zeros((COLS, PAIR), WIDE))
        sums, cols = lax.fori_loop(0, GROUP, one, start, unroll=8)
        for b in range(PER):
            out_ref[z, b * BLK:(b + 1) * BLK, :] = sums[b].astype(LOW)
        out_ref[z, ROWS:ROWS + 8, :] = tail_ref[z * PER:z * PER + 8, :].astype(LOW)
        out_ref[z, ROWS + 8:, :] = cols.astype(LOW)


def final_kernel(in_ref, gk_ref, gv_ref, gw_ref):
    total = in_ref[0].astype(WIDE)
    for z in range(1, SLOW):
        total = total + in_ref[z].astype(WIDE)
    rows = [
        total[b * BLK:(b + 1) * BLK] + total[ROWS + b:ROWS + b + 1] * (1.0 / CMP) for b in range(PER)
    ]
    turned = jnp.concatenate(rows, 0).T
    gk_ref[...] = turned[:DH]
    gv_ref[...] = turned[DH:]
    gw_ref[...] = total[ROWS + 8:]


def vmem():
    return pl.BlockSpec(memory_space=pltpu.VMEM)


def smem():
    return pl.BlockSpec(memory_space=pltpu.SMEM)


def shape(*sizes, kind=LOW):
    return jax.ShapeDtypeStruct(sizes, kind)


def local(*sizes, kind=LOW):
    return pltpu.VMEM(sizes, kind)


def inside(*arrays):
    return [pltpu.with_memory_space_constraint(array, pltpu.VMEM) for array in arrays]


def call(kernel, ins, outs, scratch=()):
    many = isinstance(outs, tuple)
    return pl.pallas_call(
        kernel,
        out_shape=outs,
        in_specs=ins,
        out_specs=tuple(vmem() for _ in outs) if many else vmem(),
        scratch_shapes=list(scratch),
        compiler_params=pltpu.CompilerParams(vmem_limit_bytes=16 << 20),
        name=kernel.__name__,
    )


def shards(queries, keys, values, hidden, log_sums, gates, branch_out, cotangent, chosen):
    place = lax.axis_index(KV)
    here = place[None]
    lists = chosen[:, 0]
    pairs, table, listing = call(
        pairs_kernel,
        [smem(), vmem(), vmem(), vmem()],
        (
            local(ROWS, PAIR),
            shape(SLOW, lists.shape[0], kind=jnp.int32),
            shape(1, lists.shape[1], kind=jnp.int32),
        ),
        (pltpu.VMEM(lists.shape, jnp.int32),),
    )(here, *[pltpu.with_memory_space_constraint(array, pltpu.HBM) for array in (keys.T, values.T, lists.T)])
    along = lax.all_gather(pairs, KV[0], axis=0, tiled=True)
    outbound = call(relay_kernel, [smem(), smem(), vmem()], local(GROUP, FETCH, PAIR))(here, table, *inside(along))
    arrived = lax.all_to_all(outbound, GROUP_AXES, split_axis=0, concat_axis=0, tiled=True)

    arrived, queries = lax.optimization_barrier((arrived, queries))
    m_sum, m_sel, ld_sum, ld_sel = call(
        prep_kernel,
        [vmem()] * 5,
        (
            local(4 * ROWS, PAIR),
            local(SUB, 4 * SUB_ROWS, PAIR),
            local(2 * ROWS, 2, kind=WIDE),
            local(SUB, 2 * SUB_ROWS, 2, kind=WIDE),
        ),
    )(queries, cotangent, jnp.transpose(gates, (0, 2, 1)), jnp.transpose(log_sums, (0, 2, 1)), branch_out)
    grad_queries, returned = call(
        main_kernel,
        [smem(), smem()] + [vmem()] * 6,
        (shape(ROWS, PAIR, kind=WIDE), local(GROUP, BACK, PAIR)),
        (pltpu.VMEM((TOPN * BLK, PAIR), LOW),),
    )(here, listing, *inside(m_sum, m_sel, ld_sum, ld_sel, arrived, hidden))
    across = lax.all_to_all(returned, GROUP_AXES, split_axis=0, concat_axis=0, tiled=True)
    merged = call(
        merge_kernel,
        [smem(), smem(), vmem()],
        local(SLOW, LAST, PAIR),
        (pltpu.VMEM((SLOW * PER + 8, PAIR), WIDE),),
    )(here, table, *inside(across))
    home = lax.all_to_all(merged, KV[0], split_axis=0, concat_axis=0, tiled=True)
    turned_keys, turned_values, grad_weight = call(
        final_kernel,
        [vmem()],
        (shape(DH, ROWS, kind=WIDE), shape(DH, ROWS, kind=WIDE), shape(COLS, PAIR, kind=WIDE)),
    )(*inside(home))
    return (grad_queries, turned_keys.T, turned_values.T, grad_weight)


def solution(mesh):
    finer = Mesh(mesh.devices.reshape(SLOW, NEAR, 8, mesh.shape["tp"]), (*KV, "tp"))
    placed = (
        P(KV, "tp"),
        P(KV, "tp"),
        P(KV, "tp"),
        P(KV, None),
        P(None, KV, "tp"),
        P(None, KV, "tp"),
        P(None, KV, "tp"),
        P(KV, "tp"),
        P(None, "tp", None),
    )
    return jax.shard_map(
        shards,
        mesh=finer,
        in_specs=placed,
        out_specs=(P(KV, "tp"), P(KV, "tp"), P(KV, "tp"), P(KV, "tp")),
        check_vma=False,
    )
```

```python
import jax
import jax.numpy as jnp
from jax import lax
from jax.experimental import pallas as pl
from jax.experimental.pallas import tpu as pltpu
from jax.sharding import Mesh
from jax.sharding import PartitionSpec as P

DH = 64
BLK = 32
TOPN = 12
SUB = 4
CMP = 32
KV = ("kv_0", "kv_1", "kv_2")
GROUP_AXES = KV[1:]
FAR = 1 << 30
WIDE = jnp.float32
LOW = jnp.bfloat16
NEAR = 4
SLOW = 16 // NEAR
GROUP = 8 * NEAR
PER = 4
PAIR = 2 * DH
ROWS = PER * BLK
SUB_ROWS = ROWS // SUB
COLS = 16
FETCH = SLOW * (BLK + PER)
SUMS = SLOW * BLK
PARTS = SLOW * (BLK + PER)
BACK = PARTS + SLOW * COLS
LAST = ROWS + 8 + COLS


def dot(a, b, ca, cb):
    return lax.dot_general(a, b, (((ca,), (cb,)), ((), ())), preferred_element_type=WIDE)


def pairs_kernel(place_ref, keys_ref, values_ref, chosen_ref, out_ref, table_ref, list_ref, turned_ref):
    both = jnp.concatenate([keys_ref[...], values_ref[...]], 0).astype(WIDE)
    out_ref[...] = both.T.astype(LOW)
    entry = chosen_ref[...]
    turned_ref[...] = entry.T
    list_ref[...] = turned_ref[pl.ds(place_ref[0], 1), :]
    own = place_ref[0] & (GROUP - 1)
    owner = jnp.where(entry >= 0, entry // PER, -1)
    inner = entry & (PER - 1)
    for z in range(SLOW):
        hit = jnp.where(owner == z * GROUP + own, inner, PER)
        table_ref[z:z + 1, :] = jnp.min(hit, 0, keepdims=True)


def relay_kernel(place_ref, table_ref, all_ref, out_ref):
    column = place_ref[0] // GROUP * GROUP
    rows = all_ref[...].astype(WIDE).reshape(SLOW * PER, CMP, PAIR)
    means = jnp.mean(rows, 1).astype(LOW)

    def one(g, carry):
        out_ref[g, SUMS:, :] = means
        for z in range(SLOW):
            pick = jnp.minimum(table_ref[z, column + g], PER - 1)
            at = pl.multiple_of((z * PER + pick) * BLK, BLK)
            out_ref[g, z * BLK:(z + 1) * BLK, :] = all_ref[pl.ds(at, BLK), :]
        return carry

    lax.fori_loop(0, GROUP, one, 0, unroll=2)


def prep_kernel(q_ref, cot_ref, gates_ref, logs_ref, out_ref, msum_ref, msel_ref, ldsum_ref, ldsel_ref):
    cols = jnp.concatenate([gates_ref[0], gates_ref[1], logs_ref[0], logs_ref[1]], 0).T
    first = lax.broadcasted_iota(jnp.int32, (ROWS, PAIR), 1) < DH
    q = q_ref[...].astype(WIDE) * (DH ** (-0.5))
    heads_q = [jnp.where(first, q, 0.0).astype(LOW), jnp.where(first, pltpu.roll(q, DH, 1), 0.0).astype(LOW)]
    cot = cot_ref[...].astype(WIDE)
    for b in range(2):
        g = jnp.where(first, cols[:, 2 * b:2 * b + 1], cols[:, 2 * b + 1:2 * b + 2]) * cot
        terms = g * out_ref[b].astype(WIDE)
        heads_g = [jnp.where(first, 0.0, pltpu.roll(g, DH, 1)).astype(LOW), jnp.where(first, 0.0, g).astype(LOW)]
        deltas = [
            jnp.sum(jnp.where(first, terms, 0.0), -1, keepdims=True),
            jnp.sum(jnp.where(first, 0.0, terms), -1, keepdims=True),
        ]
        for h in range(2):
            ld = jnp.concatenate([cols[:, 4 + 2 * b + h:5 + 2 * b + h], deltas[h]], 1)
            if b == 0:
                msum_ref[h * ROWS:(h + 1) * ROWS, :] = heads_q[h]
                msum_ref[(2 + h) * ROWS:(3 + h) * ROWS, :] = heads_g[h]
                ldsum_ref[h * ROWS:(h + 1) * ROWS, :] = ld
            else:
                for s in range(SUB):
                    here = slice(s * SUB_ROWS, (s + 1) * SUB_ROWS)
                    msel_ref[s, h * SUB_ROWS:(h + 1) * SUB_ROWS, :] = heads_q[h][here]
                    msel_ref[s, (2 + h) * SUB_ROWS:(3 + h) * SUB_ROWS, :] = heads_g[h][here]
                    ldsel_ref[s, h * SUB_ROWS:(h + 1) * SUB_ROWS, :] = ld[here]


def main_kernel(place_ref, list_ref, msum_ref, msel_ref, ldsum_ref, ldsel_ref, arr_ref, hid_ref,
                dq_ref, ret_ref, kv_ref):
    base = place_ref[0] * ROWS
    scale = DH ** (-0.5)

    def grads(m, kv, seen, ld):
        half = m.shape[0] // 2
        sd = dot(m, kv, 1, 1)
        probs = jnp.where(seen, jnp.exp(sd[:half] - ld[:, :1]), 0.0)
        ds = (probs * (sd[half:] - ld[:, 1:2])).astype(LOW)
        weights = jnp.concatenate([ds, probs.astype(LOW)], 0)
        return dot(ds, kv, 1, 0), dot(weights, m, 0, 0)

    m = msum_ref[...]
    ld = ldsum_ref[...]
    row_at = lax.broadcasted_iota(jnp.int32, (2 * ROWS, 1), 0) & (ROWS - 1)
    per_one = SLOW * PER
    step = 256 // per_one
    lane = lax.broadcasted_iota(jnp.int32, (1, step * per_one), 1)
    dq_sum = jnp.zeros((2 * ROWS, PAIR), WIDE)
    for y in range(0, GROUP, step):
        kv = jnp.concatenate([arr_ref[y + k, SUMS:, :] for k in range(step)], 0)
        owner = (lane & (per_one - 1)) // PER * GROUP + y + lane // per_one
        ends = (owner * PER + (lane & (PER - 1)) + 1) * CMP - 1 - base
        dq_part, kv_grad = grads(m, kv, ends <= row_at, ld)
        dq_sum += dq_part
        low = kv_grad.astype(LOW)
        for k in range(step):
            ret_ref[y + k, SUMS:PARTS, :] = low[k * per_one:(k + 1) * per_one]
    sub_at = lax.broadcasted_iota(jnp.int32, (2 * SUB_ROWS, 1), 0) & (SUB_ROWS - 1)
    sel_lane = lax.broadcasted_iota(jnp.int32, (1, TOPN * BLK), 1)
    for s in range(SUB):
        at_key = jnp.full((1, TOPN * BLK), FAR, jnp.int32)
        places = []
        for i in range(TOPN):
            n = list_ref[0, s * TOPN + i]
            live = n >= 0
            owner = jnp.maximum(n, 0) // PER
            fast = owner & (GROUP - 1)
            at = pl.multiple_of(owner // GROUP * BLK, BLK)
            places.append((live, fast, at))
            kv_ref[i * BLK:(i + 1) * BLK, :] = arr_ref[fast, pl.ds(at, BLK), :]
            start = jnp.where(live, n * BLK - base - i * BLK, FAR)
            at_key = jnp.where(sel_lane // BLK == i, start, at_key)
        kv = kv_ref[...]
        seen = at_key + sel_lane <= sub_at + s * SUB_ROWS
        dq_part, kv_grad = grads(msel_ref[s], kv, seen, ldsel_ref[s])
        low = kv_grad.astype(LOW)
        for i in range(TOPN):
            live, fast, at = places[i]

            @pl.when(live)
            def _(fast=fast, at=at, i=i):
                ret_ref[fast, pl.ds(at, BLK), :] = low[i * BLK:(i + 1) * BLK]

        top = s * SUB_ROWS
        for h in range(2):
            total = dq_sum[h * ROWS + top:h * ROWS + top + SUB_ROWS, :DH]
            total = total + dq_part[h * SUB_ROWS:(h + 1) * SUB_ROWS, :DH]
            dq_ref[top:top + SUB_ROWS, h * DH:(h + 1) * DH] = total * scale
    qb = dq_ref[...].astype(LOW)
    span = GROUP * COLS
    for z in range(SLOW):
        part = dot(hid_ref[:, z * span:(z + 1) * span], qb, 0, 0).astype(LOW)
        for y in range(GROUP):
            ret_ref[y, PARTS + z * COLS:PARTS + (z + 1) * COLS, :] = part[y * COLS:(y + 1) * COLS]


def merge_kernel(place_ref, table_ref, in_ref, out_ref, tail_ref):
    column = place_ref[0] // GROUP * GROUP
    tail_ref[SLOW * PER:, :] = jnp.zeros((8, PAIR), WIDE)

    def add_tail(g, tail):
        return tail + in_ref[g, SUMS:PARTS, :].astype(WIDE)

    tail_ref[:SLOW * PER, :] = lax.fori_loop(
        0, GROUP, add_tail, jnp.zeros((SLOW * PER, PAIR), WIDE), unroll=8
    )
    for z in range(SLOW):

        def one(g, carry, z=z):
            sums, cols = carry
            pick = table_ref[z, column + g]
            here = in_ref[g, z * BLK:(z + 1) * BLK, :].astype(WIDE)
            sums = tuple(sums[b] + jnp.where(pick == b, here, 0.0) for b in range(PER))
            part = in_ref[g, PARTS + z * COLS:PARTS + (z + 1) * COLS, :]
            return sums, cols + part.astype(WIDE)

        zero = jnp.zeros((BLK, PAIR), WIDE)
        start = ((zero,) * PER, jnp.zeros((COLS, PAIR), WIDE))
        sums, cols = lax.fori_loop(0, GROUP, one, start, unroll=8)
        for b in range(PER):
            out_ref[z, b * BLK:(b + 1) * BLK, :] = sums[b].astype(LOW)
        out_ref[z, ROWS:ROWS + 8, :] = tail_ref[z * PER:z * PER + 8, :].astype(LOW)
        out_ref[z, ROWS + 8:, :] = cols.astype(LOW)


def final_kernel(in_ref, gk_ref, gv_ref, gw_ref):
    total = in_ref[0].astype(WIDE)
    for z in range(1, SLOW):
        total = total + in_ref[z].astype(WIDE)
    rows = [
        total[b * BLK:(b + 1) * BLK] + total[ROWS + b:ROWS + b + 1] * (1.0 / CMP) for b in range(PER)
    ]
    turned = jnp.concatenate(rows, 0).T
    gk_ref[...] = turned[:DH]
    gv_ref[...] = turned[DH:]
    gw_ref[...] = total[ROWS + 8:]


def vmem():
    return pl.BlockSpec(memory_space=pltpu.VMEM)


def smem():
    return pl.BlockSpec(memory_space=pltpu.SMEM)


def shape(*sizes, kind=LOW):
    return jax.ShapeDtypeStruct(sizes, kind)


def local(*sizes, kind=LOW):
    return pltpu.VMEM(sizes, kind)


def inside(*arrays):
    return [pltpu.with_memory_space_constraint(array, pltpu.VMEM) for array in arrays]


def call(kernel, ins, outs, scratch=()):
    many = isinstance(outs, tuple)
    return pl.pallas_call(
        kernel,
        out_shape=outs,
        in_specs=ins,
        out_specs=tuple(vmem() for _ in outs) if many else vmem(),
        scratch_shapes=list(scratch),
        compiler_params=pltpu.CompilerParams(vmem_limit_bytes=16 << 20),
        name=kernel.__name__,
    )


def shards(queries, keys, values, hidden, log_sums, gates, branch_out, cotangent, chosen):
    place = lax.axis_index(KV)
    here = place[None]
    lists = chosen[:, 0]
    pairs, table, listing = call(
        pairs_kernel,
        [smem(), vmem(), vmem(), vmem()],
        (
            local(ROWS, PAIR),
            shape(SLOW, lists.shape[0], kind=jnp.int32),
            shape(1, lists.shape[1], kind=jnp.int32),
        ),
        (pltpu.VMEM(lists.shape, jnp.int32),),
    )(here, *[pltpu.with_memory_space_constraint(array, pltpu.HBM) for array in (keys.T, values.T, lists.T)])
    along = lax.all_gather(pairs, KV[0], axis=0, tiled=True)
    outbound = call(relay_kernel, [smem(), smem(), vmem()], local(GROUP, FETCH, PAIR))(here, table, *inside(along))
    arrived = lax.all_to_all(outbound, GROUP_AXES, split_axis=0, concat_axis=0, tiled=True)

    arrived, queries = lax.optimization_barrier((arrived, queries))
    m_sum, m_sel, ld_sum, ld_sel = call(
        prep_kernel,
        [vmem()] * 5,
        (
            local(4 * ROWS, PAIR),
            local(SUB, 4 * SUB_ROWS, PAIR),
            local(2 * ROWS, 2, kind=WIDE),
            local(SUB, 2 * SUB_ROWS, 2, kind=WIDE),
        ),
    )(queries, cotangent, jnp.transpose(gates, (0, 2, 1)), jnp.transpose(log_sums, (0, 2, 1)), branch_out)
    grad_queries, returned = call(
        main_kernel,
        [smem(), smem()] + [vmem()] * 6,
        (shape(ROWS, PAIR, kind=WIDE), local(GROUP, BACK, PAIR)),
        (pltpu.VMEM((TOPN * BLK, PAIR), LOW),),
    )(here, listing, *inside(m_sum, m_sel, ld_sum, ld_sel, arrived, hidden))
    across = lax.all_to_all(returned, GROUP_AXES, split_axis=0, concat_axis=0, tiled=True)
    merged = call(
        merge_kernel,
        [smem(), smem(), vmem()],
        local(SLOW, LAST, PAIR),
        (pltpu.VMEM((SLOW * PER + 8, PAIR), WIDE),),
    )(here, table, *inside(across))
    home = lax.all_to_all(merged, KV[0], split_axis=0, concat_axis=0, tiled=True)
    turned_keys, turned_values, grad_weight = call(
        final_kernel,
        [vmem()],
        (shape(DH, ROWS, kind=WIDE), shape(DH, ROWS, kind=WIDE), shape(COLS, PAIR, kind=WIDE)),
    )(*inside(home))
    return (grad_queries, turned_keys.T, turned_values.T, grad_weight)


def solution(mesh):
    finer = Mesh(mesh.devices.reshape(SLOW, NEAR, 8, mesh.shape["tp"]), (*KV, "tp"))
    placed = (
        P(KV, "tp"),
        P(KV, "tp"),
        P(KV, "tp"),
        P(KV, None),
        P(None, KV, "tp"),
        P(None, KV, "tp"),
        P(None, KV, "tp"),
        P(KV, "tp"),
        P(None, "tp", None),
    )
    return jax.shard_map(
        shards,
        mesh=finer,
        in_specs=placed,
        out_specs=(P(KV, "tp"), P(KV, "tp"), P(KV, "tp"), P(KV, "tp")),
        check_vma=False,
    )
```

```python
import jax
import jax.numpy as jnp
from jax import lax
from jax.experimental import pallas as pl
from jax.experimental.pallas import tpu as pltpu
from jax.sharding import Mesh
from jax.sharding import PartitionSpec as P

DH = 64
BLK = 32
TOPN = 12
SUB = 4
CMP = 32
KV = ("kv_0", "kv_1", "kv_2")
GROUP_AXES = (KV[2], KV[1])
FAR = 1 << 30
WIDE = jnp.float32
LOW = jnp.bfloat16
NEAR = 4
SLOW = 16 // NEAR
GROUP = 8 * NEAR
PER = 4
PAIR = 2 * DH
ROWS = PER * BLK
SUB_ROWS = ROWS // SUB
COLS = 16
FETCH = SLOW * (BLK + PER)
SUMS = SLOW * BLK
PARTS = SLOW * (BLK + PER)
BACK = PARTS + SLOW * COLS
LAST = ROWS + 8 + COLS


def slot(at):
    return (at & 7) * NEAR + (at >> 3)


def dot(a, b, ca, cb):
    return lax.dot_general(a, b, (((ca,), (cb,)), ((), ())), preferred_element_type=WIDE)


def pairs_kernel(place_ref, keys_ref, values_ref, chosen_ref, out_ref, table_ref, list_ref, turned_ref):
    both = jnp.concatenate([keys_ref[...], values_ref[...]], 0).astype(WIDE)
    out_ref[...] = both.T.astype(LOW)
    entry = chosen_ref[...]
    turned_ref[...] = entry.T
    list_ref[...] = turned_ref[pl.ds(place_ref[0], 1), :]
    own = place_ref[0] & (GROUP - 1)
    owner = jnp.where(entry >= 0, entry // PER, -1)
    inner = entry & (PER - 1)
    for z in range(SLOW):
        hit = jnp.where(owner == z * GROUP + own, inner, PER)
        table_ref[z:z + 1, :] = jnp.min(hit, 0, keepdims=True)


def relay_kernel(place_ref, table_ref, all_ref, out_ref):
    column = place_ref[0] // GROUP * GROUP
    rows = all_ref[...].astype(WIDE).reshape(SLOW * PER, CMP, PAIR)
    means = jnp.mean(rows, 1).astype(LOW)

    def one(g, carry):
        to = slot(g)
        out_ref[to, SUMS:, :] = means
        for z in range(SLOW):
            pick = jnp.minimum(table_ref[z, column + g], PER - 1)
            at = pl.multiple_of((z * PER + pick) * BLK, BLK)
            out_ref[to, z * BLK:(z + 1) * BLK, :] = all_ref[pl.ds(at, BLK), :]
        return carry

    lax.fori_loop(0, GROUP, one, 0, unroll=2)


def prep_kernel(q_ref, cot_ref, gates_ref, logs_ref, out_ref, msum_ref, msel_ref, ldsum_ref, ldsel_ref):
    cols = jnp.concatenate([gates_ref[0], gates_ref[1], logs_ref[0], logs_ref[1]], 0).T
    first = lax.broadcasted_iota(jnp.int32, (ROWS, PAIR), 1) < DH
    q = q_ref[...].astype(WIDE) * (DH ** (-0.5))
    heads_q = [jnp.where(first, q, 0.0).astype(LOW), jnp.where(first, pltpu.roll(q, DH, 1), 0.0).astype(LOW)]
    cot = cot_ref[...].astype(WIDE)
    for b in range(2):
        g = jnp.where(first, cols[:, 2 * b:2 * b + 1], cols[:, 2 * b + 1:2 * b + 2]) * cot
        terms = g * out_ref[b].astype(WIDE)
        heads_g = [jnp.where(first, 0.0, pltpu.roll(g, DH, 1)).astype(LOW), jnp.where(first, 0.0, g).astype(LOW)]
        deltas = [
            jnp.sum(jnp.where(first, terms, 0.0), -1, keepdims=True),
            jnp.sum(jnp.where(first, 0.0, terms), -1, keepdims=True),
        ]
        for h in range(2):
            ld = jnp.concatenate([cols[:, 4 + 2 * b + h:5 + 2 * b + h], deltas[h]], 1)
            if b == 0:
                msum_ref[h * ROWS:(h + 1) * ROWS, :] = heads_q[h]
                msum_ref[(2 + h) * ROWS:(3 + h) * ROWS, :] = heads_g[h]
                ldsum_ref[h * ROWS:(h + 1) * ROWS, :] = ld
            else:
                for s in range(SUB):
                    here = slice(s * SUB_ROWS, (s + 1) * SUB_ROWS)
                    msel_ref[s, h * SUB_ROWS:(h + 1) * SUB_ROWS, :] = heads_q[h][here]
                    msel_ref[s, (2 + h) * SUB_ROWS:(3 + h) * SUB_ROWS, :] = heads_g[h][here]
                    ldsel_ref[s, h * SUB_ROWS:(h + 1) * SUB_ROWS, :] = ld[here]


def main_kernel(place_ref, list_ref, msum_ref, msel_ref, ldsum_ref, ldsel_ref, arr_ref, hid_ref,
                dq_ref, ret_ref, kv_ref):
    base = place_ref[0] * ROWS
    after = jnp.minimum(place_ref[0] + 1, SLOW * GROUP - 1)
    spare = slot(after & (GROUP - 1))
    spare_at = after // GROUP * BLK
    scale = DH ** (-0.5)

    def grads(m, kv, seen, ld):
        half = m.shape[0] // 2
        sd = dot(m, kv, 1, 1)
        probs = jnp.where(seen, jnp.exp(sd[:half] - ld[:, :1]), 0.0)
        ds = (probs * (sd[half:] - ld[:, 1:2])).astype(LOW)
        weights = jnp.concatenate([ds, probs.astype(LOW)], 0)
        return dot(ds, kv, 1, 0), dot(weights, m, 0, 0)

    m = msum_ref[...]
    ld = ldsum_ref[...]
    row_at = lax.broadcasted_iota(jnp.int32, (2 * ROWS, 1), 0) & (ROWS - 1)
    per_one = SLOW * PER
    step = 256 // per_one
    lane = lax.broadcasted_iota(jnp.int32, (1, step * per_one), 1)
    dq_sum = jnp.zeros((2 * ROWS, PAIR), WIDE)
    for y in range(0, GROUP, step):
        kv = jnp.concatenate([arr_ref[y + k, SUMS:, :] for k in range(step)], 0)
        group = y + lane // per_one
        owner = (lane & (per_one - 1)) // PER * GROUP + (group & (NEAR - 1)) * 8 + group // NEAR
        ends = (owner * PER + (lane & (PER - 1)) + 1) * CMP - 1 - base
        dq_part, kv_grad = grads(m, kv, ends <= row_at, ld)
        dq_sum += dq_part
        low = kv_grad.astype(LOW)
        for k in range(step):
            ret_ref[y + k, SUMS:PARTS, :] = low[k * per_one:(k + 1) * per_one]
    sub_at = lax.broadcasted_iota(jnp.int32, (2 * SUB_ROWS, 1), 0) & (SUB_ROWS - 1)
    sel_lane = lax.broadcasted_iota(jnp.int32, (1, TOPN * BLK), 1)
    for s in range(SUB):
        at_key = jnp.full((1, TOPN * BLK), FAR, jnp.int32)
        places = []
        for i in range(TOPN):
            n = list_ref[0, s * TOPN + i]
            live = n >= 0
            owner = jnp.maximum(n, 0) // PER
            fast = slot(owner & (GROUP - 1))
            at = pl.multiple_of(owner // GROUP * BLK, BLK)
            places.append((live, fast, at))
            kv_ref[s, i * BLK:(i + 1) * BLK, :] = arr_ref[fast, pl.ds(at, BLK), :]
            start = jnp.where(live, n * BLK - base - i * BLK, FAR)
            at_key = jnp.where(sel_lane // BLK == i, start, at_key)
        kv = kv_ref[s]
        seen = at_key + sel_lane <= sub_at + s * SUB_ROWS
        dq_part, kv_grad = grads(msel_ref[s], kv, seen, ldsel_ref[s])
        low = kv_grad.astype(LOW)
        for i in range(TOPN):
            live, fast, at = places[i]
            fast = jnp.where(live, fast, spare)
            at = jnp.where(live, at, spare_at)
            ret_ref[fast, pl.ds(pl.multiple_of(at, BLK), BLK), :] = low[i * BLK:(i + 1) * BLK]

        top = s * SUB_ROWS
        for h in range(2):
            total = dq_sum[h * ROWS + top:h * ROWS + top + SUB_ROWS, :DH]
            total = total + dq_part[h * SUB_ROWS:(h + 1) * SUB_ROWS, :DH]
            dq_ref[top:top + SUB_ROWS, h * DH:(h + 1) * DH] = total * scale
    qb = dq_ref[...].astype(LOW)
    span = GROUP * COLS
    for z in range(SLOW):
        part = dot(hid_ref[:, z * span:(z + 1) * span], qb, 0, 0).astype(LOW)
        for y in range(GROUP):
            ret_ref[slot(y), PARTS + z * COLS:PARTS + (z + 1) * COLS, :] = part[y * COLS:(y + 1) * COLS]


def merge_kernel(place_ref, table_ref, in_ref, out_ref, tail_ref):
    column = place_ref[0] // GROUP * GROUP
    tail_ref[SLOW * PER:, :] = jnp.zeros((8, PAIR), WIDE)

    def add_tail(g, tail):
        return tail + in_ref[g, SUMS:PARTS, :].astype(WIDE)

    tail_ref[:SLOW * PER, :] = lax.fori_loop(
        0, GROUP, add_tail, jnp.zeros((SLOW * PER, PAIR), WIDE), unroll=8
    )
    for z in range(SLOW):

        def one(g, carry, z=z):
            sums, cols = carry
            here_at = slot(g)
            pick = table_ref[z, column + g]
            here = in_ref[here_at, z * BLK:(z + 1) * BLK, :].astype(WIDE)
            sums = tuple(sums[b] + jnp.where(pick == b, here, 0.0) for b in range(PER))
            part = in_ref[here_at, PARTS + z * COLS:PARTS + (z + 1) * COLS, :]
            return sums, cols + part.astype(WIDE)

        zero = jnp.zeros((BLK, PAIR), WIDE)
        start = ((zero,) * PER, jnp.zeros((COLS, PAIR), WIDE))
        sums, cols = lax.fori_loop(0, GROUP, one, start, unroll=8)
        for b in range(PER):
            out_ref[z, b * BLK:(b + 1) * BLK, :] = sums[b].astype(LOW)
        out_ref[z, ROWS:ROWS + 8, :] = tail_ref[z * PER:z * PER + 8, :].astype(LOW)
        out_ref[z, ROWS + 8:, :] = cols.astype(LOW)


def final_kernel(in_ref, gk_ref, gv_ref, gw_ref):
    total = in_ref[0].astype(WIDE)
    for z in range(1, SLOW):
        total = total + in_ref[z].astype(WIDE)
    rows = [
        total[b * BLK:(b + 1) * BLK] + total[ROWS + b:ROWS + b + 1] * (1.0 / CMP) for b in range(PER)
    ]
    turned = jnp.concatenate(rows, 0).T
    gk_ref[...] = turned[:DH]
    gv_ref[...] = turned[DH:]
    gw_ref[...] = total[ROWS + 8:]


def vmem():
    return pl.BlockSpec(memory_space=pltpu.VMEM)


def smem():
    return pl.BlockSpec(memory_space=pltpu.SMEM)


def shape(*sizes, kind=LOW):
    return jax.ShapeDtypeStruct(sizes, kind)


def local(*sizes, kind=LOW):
    return pltpu.VMEM(sizes, kind)


def inside(*arrays):
    return [pltpu.with_memory_space_constraint(array, pltpu.VMEM) for array in arrays]


def call(kernel, ins, outs, scratch=()):
    many = isinstance(outs, tuple)
    return pl.pallas_call(
        kernel,
        out_shape=outs,
        in_specs=ins,
        out_specs=tuple(vmem() for _ in outs) if many else vmem(),
        scratch_shapes=list(scratch),
        compiler_params=pltpu.CompilerParams(vmem_limit_bytes=16 << 20),
        name=kernel.__name__,
    )


def shards(queries, keys, values, hidden, log_sums, gates, branch_out, cotangent, chosen):
    place = lax.axis_index(KV)
    here = place[None]
    lists = chosen[:, 0]
    pairs, table, listing = call(
        pairs_kernel,
        [smem(), vmem(), vmem(), vmem()],
        (
            local(ROWS, PAIR),
            shape(SLOW, lists.shape[0], kind=jnp.int32),
            shape(1, lists.shape[1], kind=jnp.int32),
        ),
        (pltpu.VMEM(lists.shape, jnp.int32),),
    )(here, *[pltpu.with_memory_space_constraint(array, pltpu.HBM) for array in (keys.T, values.T, lists.T)])
    along = lax.all_gather(pairs, KV[0], axis=0, tiled=True)
    outbound = call(relay_kernel, [smem(), smem(), vmem()], local(GROUP, FETCH, PAIR))(here, table, *inside(along))
    arrived = lax.all_to_all(outbound, GROUP_AXES, split_axis=0, concat_axis=0, tiled=True)

    arrived, queries = lax.optimization_barrier((arrived, queries))
    m_sum, m_sel, ld_sum, ld_sel = call(
        prep_kernel,
        [vmem()] * 5,
        (
            local(4 * ROWS, PAIR),
            local(SUB, 4 * SUB_ROWS, PAIR),
            local(2 * ROWS, 2, kind=WIDE),
            local(SUB, 2 * SUB_ROWS, 2, kind=WIDE),
        ),
    )(queries, cotangent, jnp.transpose(gates, (0, 2, 1)), jnp.transpose(log_sums, (0, 2, 1)), branch_out)
    grad_queries, returned = call(
        main_kernel,
        [smem(), smem()] + [vmem()] * 6,
        (shape(ROWS, PAIR, kind=WIDE), local(GROUP, BACK, PAIR)),
        (pltpu.VMEM((SUB, TOPN * BLK, PAIR), LOW),),
    )(here, listing, *inside(m_sum, m_sel, ld_sum, ld_sel, arrived, hidden))
    across = lax.all_to_all(returned, GROUP_AXES, split_axis=0, concat_axis=0, tiled=True)
    merged = call(
        merge_kernel,
        [smem(), smem(), vmem()],
        local(SLOW, LAST, PAIR),
        (pltpu.VMEM((SLOW * PER + 8, PAIR), WIDE),),
    )(here, table, *inside(across))
    home = lax.all_to_all(merged, KV[0], split_axis=0, concat_axis=0, tiled=True)
    turned_keys, turned_values, grad_weight = call(
        final_kernel,
        [vmem()],
        (shape(DH, ROWS, kind=WIDE), shape(DH, ROWS, kind=WIDE), shape(COLS, PAIR, kind=WIDE)),
    )(*inside(home))
    return (grad_queries, turned_keys.T, turned_values.T, grad_weight)


def solution(mesh):
    finer = Mesh(mesh.devices.reshape(SLOW, NEAR, 8, mesh.shape["tp"]), (*KV, "tp"))
    placed = (
        P(KV, "tp"),
        P(KV, "tp"),
        P(KV, "tp"),
        P(KV, None),
        P(None, KV, "tp"),
        P(None, KV, "tp"),
        P(None, KV, "tp"),
        P(KV, "tp"),
        P(None, "tp", None),
    )
    return jax.shard_map(
        shards,
        mesh=finer,
        in_specs=placed,
        out_specs=(P(KV, "tp"), P(KV, "tp"), P(KV, "tp"), P(KV, "tp")),
        check_vma=False,
    )
```

```python
import jax
import jax.numpy as jnp
from jax import lax
from jax.experimental import pallas as pl
from jax.experimental.pallas import tpu as pltpu
from jax.sharding import Mesh
from jax.sharding import PartitionSpec as P

DH = 64
BLK = 32
TOPN = 12
SUB = 4
CMP = 32
KV = ("kv_0", "kv_1", "kv_2")
GROUP_AXES = KV[1:]
FAR = 1 << 30
WIDE = jnp.float32
LOW = jnp.bfloat16
NEAR = 4
SLOW = 16 // NEAR
GROUP = 8 * NEAR
PER = 4
PAIR = 2 * DH
ROWS = PER * BLK
SUB_ROWS = ROWS // SUB
COLS = 16
FETCH = SLOW * (BLK + PER)
SUMS = SLOW * BLK
PARTS = SLOW * (BLK + PER)
BACK = PARTS + SLOW * COLS
LAST = ROWS + 8 + COLS


def dot(a, b, ca, cb):
    return lax.dot_general(a, b, (((ca,), (cb,)), ((), ())), preferred_element_type=WIDE)


def pairs_kernel(place_ref, keys_ref, values_ref, chosen_ref, out_ref, table_ref, list_ref, turned_ref):
    both = jnp.concatenate([keys_ref[...], values_ref[...]], 0).astype(WIDE)
    out_ref[...] = both.T.astype(LOW)
    entry = chosen_ref[...]
    turned_ref[...] = entry.T
    list_ref[...] = turned_ref[pl.ds(place_ref[0], 1), :]
    own = place_ref[0] & (GROUP - 1)
    owner = jnp.where(entry >= 0, entry // PER, -1)
    inner = entry & (PER - 1)
    for z in range(SLOW):
        hit = jnp.where(owner == z * GROUP + own, inner, PER)
        table_ref[z:z + 1, :] = jnp.min(hit, 0, keepdims=True)


def relay_kernel(place_ref, table_ref, all_ref, out_ref):
    column = place_ref[0] // GROUP * GROUP
    rows = all_ref[...].astype(WIDE).reshape(SLOW * PER, CMP, PAIR)
    means = jnp.mean(rows, 1).astype(LOW)

    def one(g, carry):
        out_ref[g, SUMS:, :] = means
        for z in range(SLOW):
            pick = jnp.minimum(table_ref[z, column + g], PER - 1)
            at = pl.multiple_of((z * PER + pick) * BLK, BLK)
            out_ref[g, z * BLK:(z + 1) * BLK, :] = all_ref[pl.ds(at, BLK), :]
        return carry

    lax.fori_loop(0, GROUP, one, 0, unroll=2)


def prep_kernel(q_ref, cot_ref, gates_ref, logs_ref, out_ref, msum_ref, msel_ref, ldsum_ref, ldsel_ref):
    cols = jnp.concatenate([gates_ref[0], gates_ref[1], logs_ref[0], logs_ref[1]], 0).T
    first = lax.broadcasted_iota(jnp.int32, (ROWS, PAIR), 1) < DH
    q = q_ref[...].astype(WIDE) * (DH ** (-0.5))
    heads_q = [jnp.where(first, q, 0.0).astype(LOW), jnp.where(first, pltpu.roll(q, DH, 1), 0.0).astype(LOW)]
    cot = cot_ref[...].astype(WIDE)
    for b in range(2):
        g = jnp.where(first, cols[:, 2 * b:2 * b + 1], cols[:, 2 * b + 1:2 * b + 2]) * cot
        terms = g * out_ref[b].astype(WIDE)
        heads_g = [jnp.where(first, 0.0, pltpu.roll(g, DH, 1)).astype(LOW), jnp.where(first, 0.0, g).astype(LOW)]
        deltas = [
            jnp.sum(jnp.where(first, terms, 0.0), -1, keepdims=True),
            jnp.sum(jnp.where(first, 0.0, terms), -1, keepdims=True),
        ]
        for h in range(2):
            ld = jnp.concatenate([cols[:, 4 + 2 * b + h:5 + 2 * b + h], deltas[h]], 1)
            if b == 0:
                msum_ref[h * ROWS:(h + 1) * ROWS, :] = heads_q[h]
                msum_ref[(2 + h) * ROWS:(3 + h) * ROWS, :] = heads_g[h]
                ldsum_ref[h * ROWS:(h + 1) * ROWS, :] = ld
            else:
                for s in range(SUB):
                    here = slice(s * SUB_ROWS, (s + 1) * SUB_ROWS)
                    msel_ref[s, h * SUB_ROWS:(h + 1) * SUB_ROWS, :] = heads_q[h][here]
                    msel_ref[s, (2 + h) * SUB_ROWS:(3 + h) * SUB_ROWS, :] = heads_g[h][here]
                    ldsel_ref[s, h * SUB_ROWS:(h + 1) * SUB_ROWS, :] = ld[here]


def main_kernel(place_ref, list_ref, msum_ref, msel_ref, ldsum_ref, ldsel_ref, arr_ref, hid_ref,
                dq_ref, ret_ref, kv_ref):
    base = place_ref[0] * ROWS
    after = jnp.minimum(place_ref[0] + 1, SLOW * GROUP - 1)
    spare = after & (GROUP - 1)
    spare_at = after // GROUP * BLK
    scale = DH ** (-0.5)

    def grads(m, kv, seen, ld):
        half = m.shape[0] // 2
        sd = dot(m, kv, 1, 1)
        probs = jnp.where(seen, jnp.exp(sd[:half] - ld[:, :1]), 0.0)
        ds = (probs * (sd[half:] - ld[:, 1:2])).astype(LOW)
        weights = jnp.concatenate([ds, probs.astype(LOW)], 0)
        return dot(ds, kv, 1, 0), dot(weights, m, 0, 0)

    m = msum_ref[...]
    ld = ldsum_ref[...]
    row_at = lax.broadcasted_iota(jnp.int32, (2 * ROWS, 1), 0) & (ROWS - 1)
    per_one = SLOW * PER
    step = 256 // per_one
    lane = lax.broadcasted_iota(jnp.int32, (1, step * per_one), 1)
    dq_sum = jnp.zeros((2 * ROWS, PAIR), WIDE)
    for y in range(0, GROUP, step):
        kv = jnp.concatenate([arr_ref[y + k, SUMS:, :] for k in range(step)], 0)
        owner = (lane & (per_one - 1)) // PER * GROUP + y + lane // per_one
        ends = (owner * PER + (lane & (PER - 1)) + 1) * CMP - 1 - base
        dq_part, kv_grad = grads(m, kv, ends <= row_at, ld)
        dq_sum += dq_part
        low = kv_grad.astype(LOW)
        for k in range(step):
            ret_ref[y + k, SUMS:PARTS, :] = low[k * per_one:(k + 1) * per_one]
    sub_at = lax.broadcasted_iota(jnp.int32, (2 * SUB_ROWS, 1), 0) & (SUB_ROWS - 1)
    sel_lane = lax.broadcasted_iota(jnp.int32, (1, TOPN * BLK), 1)
    for s in range(SUB):
        at_key = jnp.full((1, TOPN * BLK), FAR, jnp.int32)
        places = []
        for i in range(TOPN):
            n = list_ref[0, s * TOPN + i]
            live = n >= 0
            owner = jnp.maximum(n, 0) // PER
            fast = owner & (GROUP - 1)
            at = pl.multiple_of(owner // GROUP * BLK, BLK)
            places.append((live, fast, at))
            kv_ref[s, i * BLK:(i + 1) * BLK, :] = arr_ref[fast, pl.ds(at, BLK), :]
            start = jnp.where(live, n * BLK - base - i * BLK, FAR)
            at_key = jnp.where(sel_lane // BLK == i, start, at_key)
        kv = kv_ref[s]
        seen = at_key + sel_lane <= sub_at + s * SUB_ROWS
        dq_part, kv_grad = grads(msel_ref[s], kv, seen, ldsel_ref[s])
        low = kv_grad.astype(LOW)
        for i in range(TOPN):
            live, fast, at = places[i]
            fast = jnp.where(live, fast, spare)
            at = jnp.where(live, at, spare_at)
            ret_ref[fast, pl.ds(pl.multiple_of(at, BLK), BLK), :] = low[i * BLK:(i + 1) * BLK]

        top = s * SUB_ROWS
        for h in range(2):
            total = dq_sum[h * ROWS + top:h * ROWS + top + SUB_ROWS, :DH]
            total = total + dq_part[h * SUB_ROWS:(h + 1) * SUB_ROWS, :DH]
            dq_ref[top:top + SUB_ROWS, h * DH:(h + 1) * DH] = total * scale
    qb = dq_ref[...].astype(LOW)
    span = GROUP * COLS
    for z in range(SLOW):
        part = dot(hid_ref[:, z * span:(z + 1) * span], qb, 0, 0).astype(LOW)
        for y in range(GROUP):
            ret_ref[y, PARTS + z * COLS:PARTS + (z + 1) * COLS, :] = part[y * COLS:(y + 1) * COLS]


def merge_kernel(place_ref, table_ref, in_ref, out_ref, tail_ref):
    column = place_ref[0] // GROUP * GROUP
    tail_ref[SLOW * PER:, :] = jnp.zeros((8, PAIR), WIDE)

    def add_tail(g, tail):
        return tail + in_ref[g, SUMS:PARTS, :].astype(WIDE)

    tail_ref[:SLOW * PER, :] = lax.fori_loop(
        0, GROUP, add_tail, jnp.zeros((SLOW * PER, PAIR), WIDE), unroll=8
    )
    for z in range(SLOW):

        def one(g, carry, z=z):
            sums, cols = carry
            pick = table_ref[z, column + g]
            here = in_ref[g, z * BLK:(z + 1) * BLK, :].astype(WIDE)
            sums = tuple(sums[b] + jnp.where(pick == b, here, 0.0) for b in range(PER))
            part = in_ref[g, PARTS + z * COLS:PARTS + (z + 1) * COLS, :]
            return sums, cols + part.astype(WIDE)

        zero = jnp.zeros((BLK, PAIR), WIDE)
        start = ((zero,) * PER, jnp.zeros((COLS, PAIR), WIDE))
        sums, cols = lax.fori_loop(0, GROUP, one, start, unroll=8)
        for b in range(PER):
            out_ref[z, b * BLK:(b + 1) * BLK, :] = sums[b].astype(LOW)
        out_ref[z, ROWS:ROWS + 8, :] = tail_ref[z * PER:z * PER + 8, :].astype(LOW)
        out_ref[z, ROWS + 8:, :] = cols.astype(LOW)


def final_kernel(in_ref, gk_ref, gv_ref, gw_ref):
    total = in_ref[0].astype(WIDE)
    for z in range(1, SLOW):
        total = total + in_ref[z].astype(WIDE)
    rows = [
        total[b * BLK:(b + 1) * BLK] + total[ROWS + b:ROWS + b + 1] * (1.0 / CMP) for b in range(PER)
    ]
    turned = jnp.concatenate(rows, 0).T
    gk_ref[...] = turned[:DH]
    gv_ref[...] = turned[DH:]
    gw_ref[...] = total[ROWS + 8:]


def vmem():
    return pl.BlockSpec(memory_space=pltpu.VMEM)


def smem():
    return pl.BlockSpec(memory_space=pltpu.SMEM)


def shape(*sizes, kind=LOW):
    return jax.ShapeDtypeStruct(sizes, kind)


def local(*sizes, kind=LOW):
    return pltpu.VMEM(sizes, kind)


def inside(*arrays):
    return [pltpu.with_memory_space_constraint(array, pltpu.VMEM) for array in arrays]


def call(kernel, ins, outs, scratch=()):
    many = isinstance(outs, tuple)
    return pl.pallas_call(
        kernel,
        out_shape=outs,
        in_specs=ins,
        out_specs=tuple(vmem() for _ in outs) if many else vmem(),
        scratch_shapes=list(scratch),
        compiler_params=pltpu.CompilerParams(vmem_limit_bytes=16 << 20),
        name=kernel.__name__,
    )


def shards(queries, keys, values, hidden, log_sums, gates, branch_out, cotangent, chosen):
    place = lax.axis_index(KV)
    here = place[None]
    lists = chosen[:, 0]
    pairs, table, listing = call(
        pairs_kernel,
        [smem(), vmem(), vmem(), vmem()],
        (
            local(ROWS, PAIR),
            shape(SLOW, lists.shape[0], kind=jnp.int32),
            shape(1, lists.shape[1], kind=jnp.int32),
        ),
        (pltpu.VMEM(lists.shape, jnp.int32),),
    )(here, *[pltpu.with_memory_space_constraint(array, pltpu.HBM) for array in (keys.T, values.T, lists.T)])
    along = lax.all_gather(pairs, KV[0], axis=0, tiled=True)
    outbound = call(relay_kernel, [smem(), smem(), vmem()], local(GROUP, FETCH, PAIR))(here, table, *inside(along))
    arrived = lax.all_to_all(outbound, GROUP_AXES, split_axis=0, concat_axis=0, tiled=True)

    arrived, queries = lax.optimization_barrier((arrived, queries))
    m_sum, m_sel, ld_sum, ld_sel = call(
        prep_kernel,
        [vmem()] * 5,
        (
            local(4 * ROWS, PAIR),
            local(SUB, 4 * SUB_ROWS, PAIR),
            local(2 * ROWS, 2, kind=WIDE),
            local(SUB, 2 * SUB_ROWS, 2, kind=WIDE),
        ),
    )(queries, cotangent, jnp.transpose(gates, (0, 2, 1)), jnp.transpose(log_sums, (0, 2, 1)), branch_out)
    grad_queries, returned = call(
        main_kernel,
        [smem(), smem()] + [vmem()] * 6,
        (shape(ROWS, PAIR, kind=WIDE), local(GROUP, BACK, PAIR)),
        (pltpu.VMEM((SUB, TOPN * BLK, PAIR), LOW),),
    )(here, listing, *inside(m_sum, m_sel, ld_sum, ld_sel, arrived, hidden))
    across = lax.all_to_all(returned, GROUP_AXES, split_axis=0, concat_axis=0, tiled=True)
    merged = call(
        merge_kernel,
        [smem(), smem(), vmem()],
        local(SLOW, LAST, PAIR),
        (pltpu.VMEM((SLOW * PER + 8, PAIR), WIDE),),
    )(here, table, *inside(across))
    home = lax.all_to_all(merged, KV[0], split_axis=0, concat_axis=0, tiled=True)
    turned_keys, turned_values, grad_weight = call(
        final_kernel,
        [vmem()],
        (shape(DH, ROWS, kind=WIDE), shape(DH, ROWS, kind=WIDE), shape(COLS, PAIR, kind=WIDE)),
    )(*inside(home))
    return (grad_queries, turned_keys.T, turned_values.T, grad_weight)


def solution(mesh):
    finer = Mesh(mesh.devices.reshape(SLOW, NEAR, 8, mesh.shape["tp"]), (*KV, "tp"))
    placed = (
        P(KV, "tp"),
        P(KV, "tp"),
        P(KV, "tp"),
        P(KV, None),
        P(None, KV, "tp"),
        P(None, KV, "tp"),
        P(None, KV, "tp"),
        P(KV, "tp"),
        P(None, "tp", None),
    )
    return jax.shard_map(
        shards,
        mesh=finer,
        in_specs=placed,
        out_specs=(P(KV, "tp"), P(KV, "tp"), P(KV, "tp"), P(KV, "tp")),
        check_vma=False,
    )
```

```python
import jax
import jax.numpy as jnp
from jax import lax
from jax.experimental import pallas as pl
from jax.experimental.pallas import tpu as pltpu
from jax.sharding import Mesh
from jax.sharding import PartitionSpec as P

DH = 64
BLK = 32
TOPN = 12
SUB = 4
CMP = 32
KV = ("kv_0", "kv_1", "kv_2")
GROUP_AXES = KV[1:]
FAR = 1 << 30
WIDE = jnp.float32
LOW = jnp.bfloat16
NEAR = 4
SLOW = 16 // NEAR
GROUP = 8 * NEAR
PER = 4
PAIR = 2 * DH
ROWS = PER * BLK
SUB_ROWS = ROWS // SUB
COLS = 16
FETCH = SLOW * (BLK + PER)
SUMS = SLOW * BLK
PARTS = SLOW * (BLK + PER)
BACK = PARTS + SLOW * COLS
LAST = ROWS + 8 + COLS


def dot(a, b, ca, cb):
    return lax.dot_general(a, b, (((ca,), (cb,)), ((), ())), preferred_element_type=WIDE)


def pairs_kernel(place_ref, keys_ref, values_ref, chosen_ref, out_ref, table_ref, list_ref, turned_ref):
    both = jnp.concatenate([keys_ref[...], values_ref[...]], 0).astype(WIDE)
    out_ref[...] = both.T.reshape(PER, BLK, PAIR).astype(LOW)
    entry = chosen_ref[...]
    turned_ref[...] = entry.T
    list_ref[...] = turned_ref[pl.ds(place_ref[0], 1), :]
    own = place_ref[0] & (GROUP - 1)
    owner = jnp.where(entry >= 0, entry // PER, -1)
    inner = entry & (PER - 1)
    for z in range(SLOW):
        hit = jnp.where(owner == z * GROUP + own, inner, PER)
        table_ref[z:z + 1, :] = jnp.min(hit, 0, keepdims=True)


def relay_kernel(place_ref, table_ref, all_ref, out_ref):
    column = place_ref[0] // GROUP * GROUP
    rows = all_ref[...].astype(WIDE)
    means = jnp.mean(rows, 1).astype(LOW)

    def one(g, carry):
        out_ref[g, SUMS:, :] = means
        for z in range(SLOW):
            pick = jnp.minimum(table_ref[z, column + g], PER - 1)
            out_ref[g, z * BLK:(z + 1) * BLK, :] = all_ref[z * PER + pick]
        return carry

    lax.fori_loop(0, GROUP, one, 0, unroll=2)


def prep_kernel(q_ref, cot_ref, gates_ref, logs_ref, out_ref, msum_ref, msel_ref, ldsum_ref, ldsel_ref):
    cols = jnp.concatenate([gates_ref[0], gates_ref[1], logs_ref[0], logs_ref[1]], 0).T
    first = lax.broadcasted_iota(jnp.int32, (ROWS, PAIR), 1) < DH
    q = q_ref[...].astype(WIDE) * (DH ** (-0.5))
    heads_q = [jnp.where(first, q, 0.0).astype(LOW), jnp.where(first, pltpu.roll(q, DH, 1), 0.0).astype(LOW)]
    cot = cot_ref[...].astype(WIDE)
    for b in range(2):
        g = jnp.where(first, cols[:, 2 * b:2 * b + 1], cols[:, 2 * b + 1:2 * b + 2]) * cot
        terms = g * out_ref[b].astype(WIDE)
        heads_g = [jnp.where(first, 0.0, pltpu.roll(g, DH, 1)).astype(LOW), jnp.where(first, 0.0, g).astype(LOW)]
        deltas = [
            jnp.sum(jnp.where(first, terms, 0.0), -1, keepdims=True),
            jnp.sum(jnp.where(first, 0.0, terms), -1, keepdims=True),
        ]
        for h in range(2):
            ld = jnp.concatenate([cols[:, 4 + 2 * b + h:5 + 2 * b + h], deltas[h]], 1)
            if b == 0:
                msum_ref[h * ROWS:(h + 1) * ROWS, :] = heads_q[h]
                msum_ref[(2 + h) * ROWS:(3 + h) * ROWS, :] = heads_g[h]
                ldsum_ref[h * ROWS:(h + 1) * ROWS, :] = ld
            else:
                for s in range(SUB):
                    here = slice(s * SUB_ROWS, (s + 1) * SUB_ROWS)
                    msel_ref[s, h * SUB_ROWS:(h + 1) * SUB_ROWS, :] = heads_q[h][here]
                    msel_ref[s, (2 + h) * SUB_ROWS:(3 + h) * SUB_ROWS, :] = heads_g[h][here]
                    ldsel_ref[s, h * SUB_ROWS:(h + 1) * SUB_ROWS, :] = ld[here]


def main_kernel(place_ref, list_ref, msum_ref, msel_ref, ldsum_ref, ldsel_ref, arr_ref, hid_ref,
                dq_ref, ret_ref, kv_ref):
    base = place_ref[0] * ROWS
    after = jnp.minimum(place_ref[0] + 1, SLOW * GROUP - 1)
    spare = after & (GROUP - 1)
    spare_at = after // GROUP * BLK
    scale = DH ** (-0.5)

    def grads(m, kv, seen, ld):
        half = m.shape[0] // 2
        sd = dot(m, kv, 1, 1)
        probs = jnp.where(seen, jnp.exp(sd[:half] - ld[:, :1]), 0.0)
        ds = (probs * (sd[half:] - ld[:, 1:2])).astype(LOW)
        weights = jnp.concatenate([ds, probs.astype(LOW)], 0)
        return dot(ds, kv, 1, 0), dot(weights, m, 0, 0)

    m = msum_ref[...]
    ld = ldsum_ref[...]
    row_at = lax.broadcasted_iota(jnp.int32, (2 * ROWS, 1), 0) & (ROWS - 1)
    per_one = SLOW * PER
    step = 256 // per_one
    lane = lax.broadcasted_iota(jnp.int32, (1, step * per_one), 1)
    dq_sum = jnp.zeros((2 * ROWS, PAIR), WIDE)
    for y in range(0, GROUP, step):
        kv = jnp.concatenate([arr_ref[y + k, SUMS:, :] for k in range(step)], 0)
        owner = (lane & (per_one - 1)) // PER * GROUP + y + lane // per_one
        ends = (owner * PER + (lane & (PER - 1)) + 1) * CMP - 1 - base
        dq_part, kv_grad = grads(m, kv, ends <= row_at, ld)
        dq_sum += dq_part
        low = kv_grad.astype(LOW)
        for k in range(step):
            ret_ref[y + k, SUMS:PARTS, :] = low[k * per_one:(k + 1) * per_one]
    sub_at = lax.broadcasted_iota(jnp.int32, (2 * SUB_ROWS, 1), 0) & (SUB_ROWS - 1)
    sel_lane = lax.broadcasted_iota(jnp.int32, (1, TOPN * BLK), 1)
    for s in range(SUB):
        at_key = jnp.full((1, TOPN * BLK), FAR, jnp.int32)
        places = []
        for i in range(TOPN):
            n = list_ref[0, s * TOPN + i]
            live = n >= 0
            owner = jnp.maximum(n, 0) // PER
            fast = owner & (GROUP - 1)
            at = pl.multiple_of(owner // GROUP * BLK, BLK)
            places.append((live, fast, at))
            kv_ref[s, i * BLK:(i + 1) * BLK, :] = arr_ref[fast, pl.ds(at, BLK), :]
            start = jnp.where(live, n * BLK - base - i * BLK, FAR)
            at_key = jnp.where(sel_lane // BLK == i, start, at_key)
        kv = kv_ref[s]
        seen = at_key + sel_lane <= sub_at + s * SUB_ROWS
        dq_part, kv_grad = grads(msel_ref[s], kv, seen, ldsel_ref[s])
        low = kv_grad.astype(LOW)
        for i in range(TOPN):
            live, fast, at = places[i]
            fast = jnp.where(live, fast, spare)
            at = jnp.where(live, at, spare_at)
            ret_ref[fast, pl.ds(pl.multiple_of(at, BLK), BLK), :] = low[i * BLK:(i + 1) * BLK]

        top = s * SUB_ROWS
        for h in range(2):
            total = dq_sum[h * ROWS + top:h * ROWS + top + SUB_ROWS, :DH]
            total = total + dq_part[h * SUB_ROWS:(h + 1) * SUB_ROWS, :DH]
            dq_ref[top:top + SUB_ROWS, h * DH:(h + 1) * DH] = total * scale
    qb = dq_ref[...].astype(LOW)
    span = GROUP * COLS
    for z in range(SLOW):
        part = dot(hid_ref[:, z * span:(z + 1) * span], qb, 0, 0).astype(LOW)
        for y in range(GROUP):
            ret_ref[y, PARTS + z * COLS:PARTS + (z + 1) * COLS, :] = part[y * COLS:(y + 1) * COLS]


def merge_kernel(place_ref, table_ref, in_ref, out_ref, tail_ref):
    column = place_ref[0] // GROUP * GROUP
    tail_ref[SLOW * PER:, :] = jnp.zeros((8, PAIR), WIDE)

    def add_tail(g, tail):
        return tail + in_ref[g, SUMS:PARTS, :].astype(WIDE)

    tail_ref[:SLOW * PER, :] = lax.fori_loop(
        0, GROUP, add_tail, jnp.zeros((SLOW * PER, PAIR), WIDE), unroll=8
    )
    for z in range(SLOW):

        def one(g, carry, z=z):
            sums, cols = carry
            pick = table_ref[z, column + g]
            here = in_ref[g, z * BLK:(z + 1) * BLK, :].astype(WIDE)
            sums = tuple(sums[b] + jnp.where(pick == b, here, 0.0) for b in range(PER))
            part = in_ref[g, PARTS + z * COLS:PARTS + (z + 1) * COLS, :]
            return sums, cols + part.astype(WIDE)

        zero = jnp.zeros((BLK, PAIR), WIDE)
        start = ((zero,) * PER, jnp.zeros((COLS, PAIR), WIDE))
        sums, cols = lax.fori_loop(0, GROUP, one, start, unroll=8)
        for b in range(PER):
            out_ref[z, b * BLK:(b + 1) * BLK, :] = sums[b].astype(LOW)
        out_ref[z, ROWS:ROWS + 8, :] = tail_ref[z * PER:z * PER + 8, :].astype(LOW)
        out_ref[z, ROWS + 8:, :] = cols.astype(LOW)


def final_kernel(in_ref, gk_ref, gv_ref, gw_ref):
    total = in_ref[0].astype(WIDE)
    for z in range(1, SLOW):
        total = total + in_ref[z].astype(WIDE)
    rows = [
        total[b * BLK:(b + 1) * BLK] + total[ROWS + b:ROWS + b + 1] * (1.0 / CMP) for b in range(PER)
    ]
    turned = jnp.concatenate(rows, 0).T
    gk_ref[...] = turned[:DH]
    gv_ref[...] = turned[DH:]
    gw_ref[...] = total[ROWS + 8:]


def vmem():
    return pl.BlockSpec(memory_space=pltpu.VMEM)


def smem():
    return pl.BlockSpec(memory_space=pltpu.SMEM)


def shape(*sizes, kind=LOW):
    return jax.ShapeDtypeStruct(sizes, kind)


def local(*sizes, kind=LOW):
    return pltpu.VMEM(sizes, kind)


def inside(*arrays):
    return [pltpu.with_memory_space_constraint(array, pltpu.VMEM) for array in arrays]


def call(kernel, ins, outs, scratch=()):
    many = isinstance(outs, tuple)
    return pl.pallas_call(
        kernel,
        out_shape=outs,
        in_specs=ins,
        out_specs=tuple(vmem() for _ in outs) if many else vmem(),
        scratch_shapes=list(scratch),
        compiler_params=pltpu.CompilerParams(vmem_limit_bytes=16 << 20),
        name=kernel.__name__,
    )


def shards(queries, keys, values, hidden, log_sums, gates, branch_out, cotangent, chosen):
    place = lax.axis_index(KV)
    here = place[None]
    lists = chosen[:, 0]
    pairs, table, listing = call(
        pairs_kernel,
        [smem(), vmem(), vmem(), vmem()],
        (
            local(PER, BLK, PAIR),
            shape(SLOW, lists.shape[0], kind=jnp.int32),
            shape(1, lists.shape[1], kind=jnp.int32),
        ),
        (pltpu.VMEM(lists.shape, jnp.int32),),
    )(here, *[pltpu.with_memory_space_constraint(array, pltpu.HBM) for array in (keys.T, values.T, lists.T)])
    along = lax.all_gather(pairs, KV[0], axis=0, tiled=True)
    outbound = call(relay_kernel, [smem(), smem(), vmem()], local(GROUP, FETCH, PAIR))(here, table, *inside(along))
    arrived = lax.all_to_all(outbound, GROUP_AXES, split_axis=0, concat_axis=0, tiled=True)

    arrived, queries = lax.optimization_barrier((arrived, queries))
    m_sum, m_sel, ld_sum, ld_sel = call(
        prep_kernel,
        [vmem()] * 5,
        (
            local(4 * ROWS, PAIR),
            local(SUB, 4 * SUB_ROWS, PAIR),
            local(2 * ROWS, 2, kind=WIDE),
            local(SUB, 2 * SUB_ROWS, 2, kind=WIDE),
        ),
    )(queries, cotangent, jnp.transpose(gates, (0, 2, 1)), jnp.transpose(log_sums, (0, 2, 1)), branch_out)
    grad_queries, returned = call(
        main_kernel,
        [smem(), smem()] + [vmem()] * 6,
        (shape(ROWS, PAIR, kind=WIDE), local(GROUP, BACK, PAIR)),
        (pltpu.VMEM((SUB, TOPN * BLK, PAIR), LOW),),
    )(here, listing, *inside(m_sum, m_sel, ld_sum, ld_sel, arrived, hidden))
    across = lax.all_to_all(returned, GROUP_AXES, split_axis=0, concat_axis=0, tiled=True)
    merged = call(
        merge_kernel,
        [smem(), smem(), vmem()],
        local(SLOW, LAST, PAIR),
        (pltpu.VMEM((SLOW * PER + 8, PAIR), WIDE),),
    )(here, table, *inside(across))
    home = lax.all_to_all(merged, KV[0], split_axis=0, concat_axis=0, tiled=True)
    turned_keys, turned_values, grad_weight = call(
        final_kernel,
        [vmem()],
        (shape(DH, ROWS, kind=WIDE), shape(DH, ROWS, kind=WIDE), shape(COLS, PAIR, kind=WIDE)),
    )(*inside(home))
    return (grad_queries, turned_keys.T, turned_values.T, grad_weight)


def solution(mesh):
    finer = Mesh(mesh.devices.reshape(SLOW, NEAR, 8, mesh.shape["tp"]), (*KV, "tp"))
    placed = (
        P(KV, "tp"),
        P(KV, "tp"),
        P(KV, "tp"),
        P(KV, None),
        P(None, KV, "tp"),
        P(None, KV, "tp"),
        P(None, KV, "tp"),
        P(KV, "tp"),
        P(None, "tp", None),
    )
    return jax.shard_map(
        shards,
        mesh=finer,
        in_specs=placed,
        out_specs=(P(KV, "tp"), P(KV, "tp"), P(KV, "tp"), P(KV, "tp")),
        check_vma=False,
    )
```
